256 devices in a mesh: ep: 64 (over z, y, core), tp: 4 (over x).
Axes of the slice: x: 4, y: 4, z: 8, core: 2. Of those that a mesh axis runs over, the one named last changes fastest.
Arguments:
- tokens: bfloat16 [1024, 2048], P('ep'), may hold values from -6 to 6
- norm_gain: float32 [2048], replicated, may hold values from 0.1 to 1.9
- query_weight: bfloat16 [2048, 1024], P(None, 'tp'), may hold values from -0.21875 to 0.21875
- key_weight: bfloat16 [2048, 512], P(None, 'tp'), may hold values from -0.125 to 0.125
- value_weight: bfloat16 [2048, 512], P(None, 'tp'), may hold values from -0.125 to 0.125
- output_weight: bfloat16 [1024, 2048], P('tp'), may hold values from -0.1875 to 0.1875
- head_gain: float32 [128], replicated, may hold values from 0.1 to 1.9
- lambdas: float32 [8], P('tp'), may hold values from 0.3 to 0.8
- key_cache: bfloat16 [1024, 1024, 4, 128], P('ep', None, 'tp')
- value_cache: bfloat16 [1024, 1024, 4, 128], P('ep', None, 'tp'), may hold values from -6 to 6
- lengths: int32 [1024], P('ep'), may hold values from 128 to 1024, as said below
- ffn_gain: float32 [2048], replicated, may hold values from 0.1 to 1.9
- routes: int32 [1024, 4], P('ep'), may hold values from 0 to 63, all different within a row; in each aligned block of 16 rows (0 to 15, 16 to 31, ...) at most 2 rows name the same one
- route_weight: float32 [1024, 4], P('ep'), may hold values from 0.1 to 1
- expert_gate: bfloat16 [64, 2048, 1024], P('ep', None, 'tp'), may hold values from -0.125 to 0.125
- expert_up: bfloat16 [64, 2048, 1024], P('ep', None, 'tp'), may hold values from -0.125 to 0.125
- expert_down: bfloat16 [64, 1024, 2048], P('ep', 'tp'), may hold values from -0.1875 to 0.1875
- dense_gate: bfloat16 [2048, 2048], P('tp'), may hold values from -0.125 to 0.125
- dense_up: bfloat16 [2048, 2048], P('tp'), may hold values from -0.125 to 0.125
- dense_down: bfloat16 [2048, 2048], P('tp'), may hold values from -0.1875 to 0.1875
- gate_vector: float32 [2048], P('tp')
Outputs:
- layer_out: bfloat16 [1024, 2048], P('ep', 'tp')
The draws below stay inside these ranges and needn't reach their ends.
Inputs may be any that keep to these rules, and one draw needn't show every extreme that they name: `routes`: each row names 4 different experts. Among the rows of one index of ep no expert is named by more than 2 rows, a bound that some block reaches. `lengths`: some sequence has length 1024. Cached positions at or past a sequence's length are not read.
All inputs are finite; a program needn't handle non-finite values.
Results may differ from the reference program's by a relative error of at most 0.015.
The reference program's roundings to bfloat16 on the way count: a program that leaves them out, or rounds other values in their place, can miss the bound.
Values may be sent and summed in bfloat16 or wider, within the bound.
A program may use at most 128 MiB of HBM per device.

```python
import math
import jax
import jax.numpy as jnp
import numpy as np
from jax import lax

D = 2048
HEADS = 8
KV_HEADS = 4
DQK = 64
DV = 128
FFE = 1024
FFD = 2048
TOPK = 4
SEQ_DEV = 16
CACHE = 1024
SEQS = 1024
EXPERTS = 64
CAP = 2
N_EP = 64
N_TP = 4


def draw_key_cache(key, part):
    normal_key = jax.random.fold_in(jax.random.fold_in(key, 11), 0)
    base_draw = jax.random.normal(normal_key, (SEQS, CACHE, KV_HEADS, 2 * DQK), jnp.float32)
    return base_draw.astype(jnp.bfloat16)


def draw_lengths(key, part):
    base_key, chosen_key = jax.random.split(jax.random.fold_in(key, 23))
    drawn = jax.random.randint(base_key, (SEQS,), CACHE // 8, CACHE + 1)
    chosen = jax.random.randint(chosen_key, (), 0, SEQS)
    return jnp.where(jnp.arange(SEQS) == chosen, CACHE, drawn).astype(jnp.int32)


def draw_gate_vector(key, part):
    inner_key = jax.random.fold_in(key, 37)
    rising = 1.0 + 3.0 * jnp.arange(FFD, dtype=jnp.float32) / FFD
    base_draw = jax.random.normal(inner_key, (FFD,), jnp.float32)
    return (base_draw * rising / math.sqrt(FFD)).astype(jnp.float32)


def with_spikes(entries, own_key, source, target, parts, factor):
    def block_of(position):
        return (jnp.arange(entries.shape[position]) // (entries.shape[position] // parts)).reshape((-1,) + (1,) * (entries.ndim - 1 - position))

    one_side = jax.random.permutation(own_key, parts)[block_of(target)]
    second = (block_of(target) + parts // 2) % parts
    return jnp.where((block_of(source) == one_side) | (block_of(source) == second), factor * entries, entries)


def levels(stream_key, dims, shards, smallest, top_value):
    level = 1.0
    for position, parts in shards:
        heights = jax.random.uniform(jax.random.fold_in(jax.random.fold_in(stream_key, 6), position), (parts,), jnp.float32, smallest / len(shards), top_value / len(shards))
        level = level * jnp.repeat(jnp.exp(heights), dims[position] // parts).reshape((-1,) + (1,) * (len(dims) - 1 - position))
    return level


def assign_block(own_key, own, number, rows, number_of, top, most, slope):
    ranking = jax.random.permutation(own_key, number_of)
    heavy_load, usual = shares(number_of, rows * top, most, slope, True), shares(number_of, rows * top, most, slope, False)
    places = jnp.arange(number_of)

    def named(sizes, rotation):
        used = int((sizes > 0).sum())
        fixed = max(1, used // 4)
        passed = fixed + (places - fixed + rotation * (used - fixed)) % max(1, number_of - fixed)
        return jnp.zeros((number_of,), jnp.int32).at[ranking[jnp.where(places < fixed, places, passed)]].set(jnp.asarray(sizes, jnp.int32))

    sizes = jnp.where(number % 4 == 0, named(heavy_load, number // 4), named(usual, number - number // 4 - 1))
    mixed = jax.random.permutation(jax.random.fold_in(own, 3), number_of)
    source_of, taker = mixed[0:number_of // 2 * 2:2], mixed[1:number_of // 2 * 2:2]
    room = jnp.minimum(sizes[source_of] - 1, most - sizes[taker]) // 2
    room = jnp.where((source_of == ranking[0]) | (taker == ranking[0]) | (sizes[taker] == 0), 0, jnp.maximum(room, 0))
    passed = jax.random.randint(jax.random.fold_in(own, 4), (number_of // 2,), 0, 1 << 20) % (room + 1)
    sizes = sizes.at[source_of].add(-passed).at[taker].add(passed)
    items = jnp.searchsorted(jnp.cumsum(sizes), jnp.arange(rows * top), side="right").astype(jnp.int32)
    listing = items.reshape(top, rows).T
    listing = listing[jax.random.permutation(jax.random.fold_in(own, 1), rows)]
    rotation = jax.random.randint(jax.random.fold_in(own, 2), (rows, 1), 0, top)
    return jnp.take_along_axis(listing, (jnp.arange(top)[None, :] + rotation) % top, axis=1)


def shares(count, total, bound, slope, full):
    loads = [(1 << 20) // math.isqrt(standing ** slope) + 1 for standing in range(1, count + 1)]
    largest = bound if full else min(bound, max(-(-total // count), total * loads[0] // sum(loads)))
    least = 1 if total - largest >= count - 1 else 0
    holding, surplus = [largest] + [least] * (count - 1), total - largest - least * (count - 1)
    while surplus > 0:
        candidates = [i for i in range(1, count) if holding[i] < largest] or [i for i in range(1, count) if holding[i] < bound]
        pool, left = sum([loads[i] for i in candidates]), surplus
        for i in candidates:
            addition = min(bound - holding[i], max(1, left * loads[i] // pool), surplus)
            holding[i] = holding[i] + addition
            surplus = surplus - addition
    return np.array(holding)


def gaussian(key, dims, width, reach, shards=(), held_as=jnp.bfloat16):
    values = jax.random.normal(key, dims, jnp.float32) * width
    if len(shards) > 0:
        values = levels(key, dims, shards, -0.22, 0.18) * values
    return jnp.clip(values, min=-reach, max=reach).astype(held_as)


def gaussian_with(stream_key, shape, width, limit, cuts, heavy, kind=jnp.bfloat16):
    values = width * jax.random.normal(stream_key, shape, jnp.float32)
    if cuts:
        values = values * levels(stream_key, shape, cuts, -0.22, 0.18)
    return jnp.clip(with_spikes(values, jax.random.fold_in(stream_key, 3), *heavy), -limit, limit).astype(kind)


def setup_inputs(seed: int = 0) -> dict:
    key_of = jax.random.split(jax.random.key(seed), 22)
    tokens = gaussian(key_of[0], (SEQS, D), 1.0, 6.0, ((0, 64),))
    norm_gain = jnp.clip(1.0 + 0.18 * jax.random.normal(key_of[1], (D,), jnp.float32), 0.1, 1.9)
    query_weight = gaussian(key_of[2], (D, HEADS * 2 * DQK), (D // 3) ** -0.5, 0.21875, ((1, 4),))
    key_weight = gaussian(key_of[3], (D, KV_HEADS * 2 * DQK), D ** -0.5, 0.125, ((1, 4),))
    value_weight = gaussian(key_of[4], (D, KV_HEADS * DV), D ** -0.5, 0.125, ((1, 4),))
    output_weight = gaussian(key_of[5], (HEADS * DV, D), (HEADS * DV) ** -0.5, 0.1875, ((0, 4),))
    head_gain = jnp.clip(1.0 + 0.18 * jax.random.normal(key_of[6], (DV,), jnp.float32), 0.1, 1.9)
    lambdas = jnp.clip(0.3 + 0.5 * jax.random.uniform(key_of[7], (HEADS,), jnp.float32) ** levels(key_of[7], (HEADS,), ((0, 4),), -0.2, 0.2), 0.3, 0.8)
    key_cache = draw_key_cache(jax.random.fold_in(key_of[21], 71), 0)
    value_cache = gaussian(key_of[9], (SEQS, CACHE, KV_HEADS, DV), 1.0, 6.0, ((0, 64), (2, 4)))
    lengths = draw_lengths(jax.random.fold_in(key_of[21], 71), 0)
    ffn_gain = jnp.clip(1.0 + 0.18 * jax.random.normal(key_of[11], (D,), jnp.float32), 0.1, 1.9)
    routes_keys = jax.random.split(jax.random.fold_in(key_of[12], 1), SEQS // SEQ_DEV)
    routes_turns = jax.random.permutation(jax.random.fold_in(key_of[12], 3), SEQS // SEQ_DEV)
    routes = jax.vmap(lambda own, number: assign_block(jax.random.fold_in(key_of[12], 2), own, number, SEQ_DEV, EXPERTS, TOPK, CAP, 2))(routes_keys, routes_turns).reshape((SEQS, TOPK))
    route_weight = jnp.clip(0.1 + 0.9 * jax.random.uniform(key_of[13], (SEQS, TOPK), jnp.float32) ** levels(key_of[13], (SEQS, TOPK), ((0, 64),), -0.2, 0.2), 0.1, 1.0)
    expert_gate = gaussian(key_of[14], (EXPERTS, D, FFE), D ** -0.5, 0.125, ((0, 64), (2, 4)))
    expert_up = gaussian(key_of[15], (EXPERTS, D, FFE), D ** -0.5, 0.125, ((0, 64), (2, 4)))
    expert_down = gaussian(key_of[16], (EXPERTS, FFE, D), FFE ** -0.5, 0.1875, ((0, 64), (1, 4)))
    dense_gate = gaussian(key_of[17], (FFD, D), D ** -0.5, 0.125, ((0, 4),))
    dense_up = gaussian(key_of[18], (FFD, D), D ** -0.5, 0.125, ((0, 4),))
    dense_down = gaussian_with(key_of[19], (FFD, D), FFD ** -0.5, 0.1875, ((0, 4),), (0, 1, 4, 2.0))
    gate_vector = draw_gate_vector(jax.random.fold_in(key_of[21], 71), 0)
    return {"tokens": tokens, "norm_gain": norm_gain, "query_weight": query_weight, "key_weight": key_weight, "value_weight": value_weight, "output_weight": output_weight, "head_gain": head_gain, "lambdas": lambdas, "key_cache": key_cache, "value_cache": value_cache, "lengths": lengths, "ffn_gain": ffn_gain, "routes": routes, "route_weight": route_weight, "expert_gate": expert_gate, "expert_up": expert_up, "expert_down": expert_down, "dense_gate": dense_gate, "dense_up": dense_up, "dense_down": dense_down, "gate_vector": gate_vector}


epsilon = 1e-06

def rms_scale(values, gain):
    return values * lax.rsqrt(lax.optimization_barrier(jnp.mean(values * values, axis=-1, keepdims=True)) + epsilon) * gain

def diff_attend(queries, new_key, new_value, key_rows, value_rows, length, lambda_grid):
    score_scale = DQK ** (-0.5)
    query_wide = queries.astype(jnp.float32)
    cache_scores = jnp.einsum('kgmd,ckmd->kgmc', query_wide, key_rows.astype(jnp.float32)) * score_scale
    own_score = jnp.einsum('kgmd,kmd->kgm', query_wide, new_key.astype(jnp.float32)) * score_scale
    live_mask = jnp.arange(CACHE) < length
    cache_scores = jnp.where(live_mask, cache_scores, -jnp.inf)
    top_score = jnp.maximum(lax.optimization_barrier(jnp.max(cache_scores, axis=-1)), own_score)
    cache_exp = jnp.exp(cache_scores - top_score[..., None])
    own_exp = jnp.exp(own_score - top_score)
    totals = lax.optimization_barrier(jnp.sum(cache_exp, axis=-1)) + own_exp
    cache_prob = cache_exp / totals[..., None]
    own_prob = own_exp / totals
    cache_weight = (cache_prob[:, :, 0] - lambda_grid[..., None] * cache_prob[:, :, 1]).astype(jnp.bfloat16)
    own_weight = (own_prob[:, :, 0] - lambda_grid * own_prob[:, :, 1]).astype(jnp.bfloat16)
    mixture = jnp.einsum('kgc,ckv->kgv', cache_weight.astype(jnp.float32), value_rows.astype(jnp.float32))
    return mixture + own_weight.astype(jnp.float32)[..., None] * new_value.astype(jnp.float32)[:, None, :]

def reference(tokens, norm_gain, query_weight, key_weight, value_weight, output_weight, head_gain, lambdas, key_cache, value_cache, lengths, ffn_gain, routes, route_weight, expert_gate, expert_up, expert_down, dense_gate, dense_up, dense_down, gate_vector):
    group_size = HEADS // KV_HEADS
    tokens_wide = tokens.astype(jnp.float32)
    normed = rms_scale(tokens_wide, norm_gain).astype(jnp.bfloat16)
    queries = jnp.dot(normed, query_weight, preferred_element_type=jnp.float32).astype(jnp.bfloat16)
    new_keys = jnp.dot(normed, key_weight, preferred_element_type=jnp.float32).astype(jnp.bfloat16)
    new_values = jnp.dot(normed, value_weight, preferred_element_type=jnp.float32).astype(jnp.bfloat16)
    queries = queries.reshape(SEQS, KV_HEADS, group_size, 2, DQK)
    new_keys = new_keys.reshape(SEQS, KV_HEADS, 2, DQK)
    new_values = new_values.reshape(SEQS, KV_HEADS, DV)
    lambda_grid = lambdas.reshape(KV_HEADS, group_size)

    def one_sequence(inputs):
        seq_query, seq_key, seq_value, seq_keys, seq_values, seq_length = inputs
        return diff_attend(seq_query, seq_key, seq_value, seq_keys.reshape(CACHE, KV_HEADS, 2, DQK), seq_values, seq_length, lambda_grid)
    mixture = lax.map(one_sequence, (queries, new_keys, new_values, key_cache, value_cache, lengths))
    head_rows = rms_scale(mixture, head_gain).astype(jnp.bfloat16).reshape(SEQS, HEADS * DV)
    block_rows = HEADS * DV // N_TP
    attention = jnp.zeros((SEQS, D), jnp.float32)
    for quarter in range(N_TP):
        partial_value = jnp.dot(head_rows[:, quarter * block_rows:(quarter + 1) * block_rows], output_weight[quarter * block_rows:(quarter + 1) * block_rows], preferred_element_type=jnp.float32)
        attention = attention + lax.optimization_barrier(partial_value.astype(jnp.bfloat16)).astype(jnp.float32)
    residual = tokens_wide + attention
    ffn_in = rms_scale(residual, ffn_gain).astype(jnp.bfloat16)
    gate_pre = jnp.dot(ffn_in, dense_gate.T, preferred_element_type=jnp.float32)
    up_proj = jnp.dot(ffn_in, dense_up.T, preferred_element_type=jnp.float32)
    dense_hidden = (jax.nn.silu(gate_pre) * up_proj).astype(jnp.bfloat16)
    gate_logit = lax.optimization_barrier(jnp.sum(dense_hidden.astype(jnp.float32) * gate_vector, axis=-1))
    dense_sum = jnp.dot(dense_hidden, dense_down, preferred_element_type=jnp.float32)
    dense_out = jax.nn.sigmoid(gate_logit)[:, None] * dense_sum
    pair_expert = routes.reshape(-1).astype(jnp.int32)
    onehot = (pair_expert[:, None] == jnp.arange(EXPERTS, dtype=jnp.int32)[None, :]).astype(jnp.int32)
    running = jnp.cumsum(onehot.reshape(N_EP, SEQ_DEV * TOPK, EXPERTS), axis=1).reshape(SEQS * TOPK, EXPERTS)
    slot_rank = lax.optimization_barrier(jnp.sum(running * onehot, axis=1)) - 1
    group_index = jnp.arange(SEQS * TOPK, dtype=jnp.int32) // (SEQ_DEV * TOPK)
    column = (group_index * CAP + slot_rank).astype(jnp.int32)
    token_of_pair = jnp.arange(SEQS * TOPK, dtype=jnp.int32) // TOPK
    buffer = jnp.zeros((EXPERTS, N_EP * CAP, D), jnp.bfloat16).at[pair_expert, column].set(ffn_in[token_of_pair])

    def expert_apply(inputs):
        row_block, w_gate, w_up, w_down = inputs
        expert_pre = jnp.dot(row_block, w_gate, preferred_element_type=jnp.float32)
        expert_upper = jnp.dot(row_block, w_up, preferred_element_type=jnp.float32)
        expert_hidden = (jax.nn.silu(expert_pre) * expert_upper).astype(jnp.bfloat16)
        quarter_width = FFE // N_TP
        summed = jnp.zeros((row_block.shape[0], D), jnp.float32)
        for quarter in range(N_TP):
            partial_value = jnp.dot(expert_hidden[:, quarter * quarter_width:(quarter + 1) * quarter_width], w_down[quarter * quarter_width:(quarter + 1) * quarter_width], preferred_element_type=jnp.float32)
            summed = summed + lax.optimization_barrier(partial_value.astype(jnp.bfloat16)).astype(jnp.float32)
        return summed.astype(jnp.bfloat16)
    expert_rows = lax.map(expert_apply, (buffer, expert_gate, expert_up, expert_down))
    picked = expert_rows[pair_expert, column].reshape(SEQS, TOPK, D).astype(jnp.float32)
    expert_mix = lax.optimization_barrier(jnp.sum(picked * route_weight[:, :, None], axis=1))
    return (residual + expert_mix + dense_out).astype(jnp.bfloat16)
```

```python
import jax
import jax.numpy as jnp
from jax import lax
from jax.experimental import pallas as pl
from jax.experimental.pallas import tpu as pltpu
from jax.sharding import PartitionSpec as P

MESH = pl.DeviceIdType.MESH
BF = jnp.bfloat16
F32 = jnp.float32
EPS = 1e-06

SEQ = 16
D = 2048
QUARTER = 512
CACHE = 1024
NZ, NY, NC, NX = 8, 4, 2, 4
PEERS = NZ * NY * NC
ROWS = 2 * PEERS
ORDER = (0, 1, 7, 2, 6, 3, 5, 4)
PLACE = {dz: p for p, dz in enumerate(ORDER)}
CHUNKS = 4
CHUNK = ROWS // CHUNKS
GROUP = ROWS // NZ
BATCH = 4


def offsets(block):
    p, j = divmod(block, NY * NC)
    return ORDER[p], j // NC, j % NC


def opposite(block):
    dz, dy, dc = offsets(block)
    return PLACE[(NZ - dz) % NZ] * (NY * NC) + ((NY - dy) % NY) * NC + dc


def mm(a, b):
    return jnp.dot(a, b, preferred_element_type=F32)


def mm_t(a, b):
    return lax.dot_general(a, b, (((1,), (1,)), ((), ())), preferred_element_type=F32)


def silu(v):
    return v * (1.0 / (1.0 + jnp.exp(-v)))


def kernel(
    lambdas, lengths,
    tokens_h, norm_gain_h, wq_h, wk_h, wv_h, wo_h, head_gain_h, kc_h, vc_h, ffn_gain_h,
    routes_h, route_weight_h, eg_h, eu_h, ed_h, dg_h, du_h, dd_h, gate_h,
    out_ref,
    tok, ng, wq, wk, wv, wo, hg, kc, vc, fg, rt, rw, eg, eu, ed, dg, du, dd, gv,
    qs, own, nv, sc, ho, part1, ffn, outb, big, eparts, rs, rout, ret, dsend, drecv, gl, tick,
    load, kload, vload,
    p_send, p_recv, d_send, d_recv, ag_send, ag_recv, rs_send, rs_recv, b_send, b_recv,
    ds_send, ds_recv, g_send, g_recv,
):
    me = lax.axis_index("ep")
    x = lax.axis_index("tp")
    z, y, c = me // (NY * NC), (me // NC) % NY, me % NC

    def ep_at(block):
        dz, dy, dc = offsets(block)
        return ((z + dz) % NZ) * (NY * NC) + ((y + dy) % NY) * NC + (c + dc) % NC

    def messages(count, sem):
        size = tick.at[pl.ds(0, count)]
        pltpu.make_async_copy(size, size, sem).wait()

    loads = []

    def fetch(src, dst):
        copy = pltpu.make_async_copy(src, dst, load.at[len(loads)])
        copy.start()
        loads.append(copy)
        return copy

    l_tok = fetch(tokens_h, tok)
    l_ng = fetch(norm_gain_h, ng)
    l_wq = fetch(wq_h, wq)
    l_wk = fetch(wk_h, wk)
    l_wv = fetch(wv_h, wv)
    l_rt = fetch(routes_h, rt)
    l_rw = fetch(route_weight_h, rw)
    l_hg = fetch(head_gain_h, hg)
    l_fg = fetch(ffn_gain_h, fg)
    l_gv = fetch(gate_h, gv)
    for i in range(SEQ // BATCH):
        pltpu.make_async_copy(
            kc_h.at[pl.ds(i * BATCH, BATCH)], kc.at[pl.ds(i * BATCH, BATCH)], kload.at[i]
        ).start()
    for i in range(SEQ // BATCH):
        pltpu.make_async_copy(
            vc_h.at[pl.ds(i * BATCH, BATCH)], vc.at[pl.ds(i * BATCH, BATCH)], vload.at[i]
        ).start()
    l_wo = fetch(wo_h, wo)
    l_dg = fetch(dg_h, dg)
    l_du = fetch(du_h, du)
    l_dd = fetch(dd_h, dd)
    l_eg = fetch(eg_h, eg)
    l_eu = fetch(eu_h, eu)
    l_ed = fetch(ed_h, ed)

    barrier = pltpu.get_barrier_semaphore()

    @pl.loop(1, PEERS)
    def _(i):
        pl.semaphore_signal(barrier, inc=1, device_id=((me + i) % PEERS, x), device_id_type=MESH)

    @pl.loop(1, NX)
    def _(i):
        pl.semaphore_signal(barrier, inc=1, device_id=(me, (x + i) % NX), device_id_type=MESH)

    l_rt.wait()
    l_rw.wait()
    routes = rt[...]
    dz = ((routes >> 3) - z) & 7
    place = jnp.where(dz == 0, 0, jnp.where(dz <= 4, 2 * dz - 1, 16 - 2 * dz))
    dy = ((routes >> 1) - y) & 3
    dc = (routes - c) & 1
    rel = place * 8 + dy * 2 + dc
    row = lax.broadcasted_iota(jnp.int32, (ROWS, SEQ), 0)
    named = jnp.zeros((ROWS, SEQ), F32)
    weighted = jnp.zeros((ROWS, SEQ), F32)
    weights = rw[...]
    for k in range(4):
        hit = (row >> 1) == rel[k : k + 1, :]
        named = named + jnp.where(hit, 1.0, 0.0)
        weighted = weighted + jnp.where(hit, weights[k : k + 1, :], 0.0)
    before = lax.broadcasted_iota(jnp.int32, (SEQ, SEQ), 0) < lax.broadcasted_iota(
        jnp.int32, (SEQ, SEQ), 1
    )
    rank = mm(named.astype(BF), jnp.where(before, 1.0, 0.0).astype(BF))
    mine = jnp.abs(rank - (row & 1).astype(F32)) < 0.5
    dispatch = jnp.where(mine, named, 0.0).astype(BF)
    combine = jnp.where(mine, weighted, 0.0)

    l_tok.wait()
    l_ng.wait()
    wide = tok[...].astype(F32)
    scale = lax.rsqrt(jnp.mean(wide * wide, axis=-1, keepdims=True) + EPS)
    normed = (wide * scale * ng[...]).astype(BF)
    l_wq.wait()
    l_wk.wait()
    l_wv.wait()
    queries = mm(normed, wq[...]).astype(BF).astype(F32) * 0.125
    new_keys = mm(normed, wk[...]).astype(BF).astype(F32)
    nv[...] = mm(normed, wv[...]).astype(BF).astype(F32)
    low = lax.broadcasted_iota(jnp.int32, (SEQ, 128), 1) < 64
    for m in range(2):
        for g in range(2):
            head = queries[:, g * 128 : (g + 1) * 128]
            head = jnp.where(low, head, 0.0) if m == 0 else jnp.where(low, 0.0, head)
            r = (m * 2 + g) * SEQ
            qs[r : r + SEQ, :] = head
            score = jnp.sum(head * new_keys, axis=-1, keepdims=True)
            own[r : r + SEQ, :] = jnp.broadcast_to(score, (SEQ, 128))
    qs[4 * SEQ :, :] = jnp.zeros((4 * SEQ, 128), F32)
    own[4 * SEQ :, :] = jnp.zeros((4 * SEQ, 128), F32)

    @pl.loop(0, SEQ // BATCH)
    def _(i):
        pltpu.make_async_copy(
            kc_h.at[pl.ds(i * BATCH, BATCH)], kc.at[pl.ds(i * BATCH, BATCH)], kload.at[i]
        ).wait()
        for b in range(BATCH):
            s = i * BATCH + b
            q8 = qs[pl.ds(s, 8, stride=SEQ), :].astype(BF)
            sc[s] = mm_t(q8, kc[s])

    head_row = lax.broadcasted_iota(jnp.int32, (8, 1), 0)
    sign = jnp.where(head_row < 2, 1.0, jnp.where(head_row == 2, -lambdas[0], -lambdas[1]))
    sign = jnp.where(head_row < 4, sign, 0.0)
    position = lax.broadcasted_iota(jnp.int32, (8, CACHE), 1)

    @pl.loop(0, SEQ // BATCH)
    def _(i):
        pltpu.make_async_copy(
            vc_h.at[pl.ds(i * BATCH, BATCH)], vc.at[pl.ds(i * BATCH, BATCH)], vload.at[i]
        ).wait()
        for b in range(BATCH):
            s = i * BATCH + b
            scores = jnp.where(position < lengths[s], sc[s], -jnp.inf)
            own_score = own[pl.ds(s, 8, stride=SEQ), :][:, 0:1]
            top = jnp.maximum(jnp.max(scores, axis=-1, keepdims=True), own_score)
            probs = jnp.exp(scores - top)
            own_prob = jnp.exp(own_score - top)
            total = jnp.sum(probs, axis=-1, keepdims=True) + own_prob
            factor = sign / total
            probs = probs * factor
            own_prob = own_prob * factor
            attend = (probs + pltpu.roll(probs, 6, 0)).astype(BF)
            own_weight = (own_prob[0:2] + own_prob[2:4]).astype(BF).astype(F32)
            mixed = mm(attend, vc[s])[0:2] + own_weight * nv[pl.ds(s, 1), :]
            ho[pl.ds(s, 1), :] = mixed[0:1]
            ho[pl.ds(SEQ + s, 1), :] = mixed[1:2]

    l_hg.wait()
    heads = ho[...]
    heads = heads * lax.rsqrt(jnp.mean(heads * heads, axis=-1, keepdims=True) + EPS) * hg[...]
    heads = heads.astype(BF)
    l_wo.wait()
    part1[0] = (mm(heads[:SEQ], wo[0:128, :]) + mm(heads[SEQ:], wo[128:256, :])).astype(BF)

    pl.semaphore_wait(barrier, PEERS - 1 + NX - 1)

    def along_tp(r, src, dst, send, recv):
        return pltpu.make_async_remote_copy(
            src_ref=src, dst_ref=dst, send_sem=send, recv_sem=recv,
            device_id=(me, (x + r) % NX), device_id_type=MESH,
        )

    shares = []
    for r in (2, 1, 3):
        copy = along_tp(r, part1.at[0], part1.at[NX - r], p_send.at[r], p_recv.at[NX - r])
        copy.start()
        shares.append(copy)
    l_fg.wait()
    for r in (1, 3, 2):
        pltpu.make_async_copy(part1.at[r], part1.at[r], p_recv.at[r]).wait()
    total = part1[0].astype(F32)
    for r in (1, 2, 3):
        total = total + part1[r].astype(F32)
    residual = wide + total
    scale = lax.rsqrt(jnp.mean(residual * residual, axis=-1, keepdims=True) + EPS)
    ffn_in = (residual * scale * fg[...]).astype(BF)
    mine_at = pl.multiple_of(x * QUARTER, QUARTER)
    ffn[...] = ffn_in

    routed = mm(dispatch, ffn[:, pl.ds(mine_at, QUARTER)]).astype(BF)
    outb[...] = routed
    big[0, 0:2, :] = routed[0:2]
    for block in range(1, PEERS):
        there = opposite(block)
        pltpu.make_async_remote_copy(
            src_ref=outb.at[pl.ds(2 * block, 2), :],
            dst_ref=big.at[0, pl.ds(2 * there, 2), :],
            send_sem=d_send,
            recv_sem=d_recv.at[there // (NY * NC)],
            device_id=(ep_at(block), x),
            device_id_type=MESH,
        ).start()

    l_gv.wait()
    l_dg.wait()
    gate_pre = mm_t(ffn_in, dg[...])
    l_du.wait()
    hidden = (silu(gate_pre) * mm_t(ffn_in, du[...])).astype(BF)
    logit = jnp.sum(hidden.astype(F32) * gv[...], axis=-1, keepdims=True)
    gl[0] = jnp.broadcast_to(logit, (SEQ, 128))
    l_dd.wait()
    for r in range(NX):
        at = pl.multiple_of(((x + r) % NX) * QUARTER, QUARTER)
        dsend[r] = mm(hidden, dd[:, pl.ds(at, QUARTER)]).astype(BF)
    for r in (2, 1, 3):
        copy = along_tp(r, dsend.at[r], drecv.at[NX - r], ds_send.at[r], ds_recv.at[NX - r])
        copy.start()
        shares.append(copy)
        copy = along_tp(r, gl.at[0], gl.at[NX - r], g_send.at[r], g_recv.at[NX - r])
        copy.start()
        shares.append(copy)

    def arrived(ch):
        for p in (2 * ch, 2 * ch + 1):
            messages(GROUP // 2 - (p == 0), d_recv.at[p])
        rows = pl.ds(ch * CHUNK, CHUNK)
        for r in (2, 1, 3):
            copy = along_tp(
                r, big.at[0, rows, :], big.at[NX - r, rows, :],
                ag_send.at[ch, r], ag_recv.at[ch, NX - r],
            )
            copy.start()
            shares.append(copy)

    def work(ch):
        rows = pl.ds(ch * CHUNK, CHUNK)
        for r in (1, 3, 2):
            block = big.at[r, rows, :]
            pltpu.make_async_copy(block, block, ag_recv.at[ch, r]).wait()
        pre = jnp.zeros((CHUNK, 256), F32)
        up = jnp.zeros((CHUNK, 256), F32)
        for r in range(NX):
            at = pl.ds(pl.multiple_of(((x + r) % NX) * QUARTER, QUARTER), QUARTER)
            block = big[r, rows, :]
            pre = pre + mm(block, eg[at, :])
            up = up + mm(block, eu[at, :])
        hidden = (silu(pre) * up).astype(BF)
        for r in range(NX):
            at = pl.ds(pl.multiple_of(((x + r) % NX) * QUARTER, QUARTER), QUARTER)
            eparts[r, rows, :] = mm(hidden, ed[:, at]).astype(BF)
        for r in (2, 1, 3):
            copy = along_tp(
                r, eparts.at[r, rows, :], rs.at[NX - r, rows, :],
                rs_send.at[ch, r], rs_recv.at[ch, NX - r],
            )
            copy.start()
            shares.append(copy)

    def give_back(ch):
        rows = pl.ds(ch * CHUNK, CHUNK)
        for r in (1, 3, 2):
            block = rs.at[r, rows, :]
            pltpu.make_async_copy(block, block, rs_recv.at[ch, r]).wait()
        total = eparts[0, rows, :].astype(F32)
        for r in (1, 2, 3):
            total = total + rs[r, rows, :].astype(F32)
        total = total.astype(BF)
        rout[rows, :] = total
        if ch == 0:
            ret[0:2, :] = total[0:2]
        for block in range(ch * CHUNK // 2, (ch + 1) * CHUNK // 2):
            if block:
                pltpu.make_async_remote_copy(
                    src_ref=rout.at[pl.ds(2 * block, 2), :],
                    dst_ref=ret.at[pl.ds(2 * opposite(block), 2), :],
                    send_sem=b_send,
                    recv_sem=b_recv,
                    device_id=(ep_at(block), x),
                    device_id_type=MESH,
                ).start()

    arrived(0)
    arrived(1)
    l_eg.wait()
    l_eu.wait()
    l_ed.wait()
    arrived(2)
    arrived(3)
    work(1)
    work(2)
    give_back(1)
    work(3)
    give_back(2)
    work(0)
    give_back(3)
    give_back(0)

    for r in (1, 3, 2):
        pltpu.make_async_copy(drecv.at[r], drecv.at[r], ds_recv.at[r]).wait()
        pltpu.make_async_copy(gl.at[r], gl.at[r], g_recv.at[r]).wait()
    dense = dsend[0].astype(F32)
    logit = gl[0]
    for r in (1, 2, 3):
        dense = dense + drecv[r].astype(F32)
        logit = logit + gl[r]
    gate = 1.0 / (1.0 + jnp.exp(-logit[:, 0:1]))
    kept = tok[:, pl.ds(mine_at, QUARTER)].astype(F32)
    for r in range(NX):
        kept = kept + part1[r, :, pl.ds(mine_at, QUARTER)].astype(F32)
    kept = kept + gate * dense
    coarse = combine.astype(BF)
    fine = (combine - coarse.astype(F32)).astype(BF)

    messages(PEERS - 1, b_recv)
    back = ret[...]
    over = (((0,), (0,)), ((), ()))
    mix = lax.dot_general(coarse, back, over, preferred_element_type=F32)
    mix = mix + lax.dot_general(fine, back, over, preferred_element_type=F32)
    out_ref[...] = (kept + mix).astype(BF)

    for copy in shares:
        copy.wait_send()
    messages(PEERS - 1, d_send)
    messages(PEERS - 1, b_send)


def shards(
    tokens, norm_gain, query_weight, key_weight, value_weight, output_weight, head_gain, lambdas,
    key_cache, value_cache, lengths, ffn_gain, routes, route_weight, expert_gate, expert_up,
    expert_down, dense_gate, dense_up, dense_down, gate_vector,
):
    hbm = pl.BlockSpec(memory_space=pl.ANY)
    smem = pl.BlockSpec(memory_space=pltpu.SMEM)
    vm = pltpu.VMEM
    dma = pltpu.SemaphoreType.DMA
    return pl.pallas_call(
        kernel,
        name="layer",
        out_shape=jax.ShapeDtypeStruct((SEQ, QUARTER), BF),
        in_specs=[smem, smem] + [hbm] * 19,
        out_specs=pl.BlockSpec(memory_space=pltpu.VMEM),
        scratch_shapes=[
            vm((SEQ, D), BF), vm((1, D), F32), vm((D, 256), BF), vm((D, 128), BF), vm((D, 128), BF),
            vm((256, D), BF), vm((1, 128), F32), vm((SEQ, CACHE, 128), BF), vm((SEQ, CACHE, 128), BF),
            vm((1, D), F32), vm((4, SEQ), jnp.int32), vm((4, SEQ), F32),
            vm((D, 256), BF), vm((D, 256), BF), vm((256, D), BF),
            vm((512, D), BF), vm((512, D), BF), vm((512, D), BF), vm((1, 512), F32),
            vm((8 * SEQ, 128), F32), vm((8 * SEQ, 128), F32), vm((SEQ, 128), F32),
            vm((SEQ, 8, CACHE), F32), vm((2 * SEQ, 128), F32),
            vm((NX, SEQ, D), BF), vm((SEQ, D), BF), vm((ROWS, QUARTER), BF),
            vm((NX, ROWS, QUARTER), BF), vm((NX, ROWS, QUARTER), BF), vm((NX, ROWS, QUARTER), BF),
            vm((ROWS, QUARTER), BF), vm((ROWS, QUARTER), BF),
            vm((NX, SEQ, QUARTER), BF), vm((NX, SEQ, QUARTER), BF), vm((NX, SEQ, 128), F32),
            vm((PEERS, 8, 128), BF),
            dma((17,)), dma((SEQ // BATCH,)), dma((SEQ // BATCH,)),
            dma((NX,)), dma((NX,)), dma, dma((NZ,)), dma((CHUNKS, NX)), dma((CHUNKS, NX)),
            dma((CHUNKS, NX)), dma((CHUNKS, NX)), dma, dma,
            dma((NX,)), dma((NX,)), dma((NX,)), dma((NX,)),
        ],
        compiler_params=pltpu.CompilerParams(
            collective_id=0, has_side_effects=True, vmem_limit_bytes=60 * 1024 * 1024
        ),
    )(
        lambdas, lengths,
        tokens, norm_gain.reshape(1, D), query_weight, key_weight, value_weight, output_weight,
        head_gain.reshape(1, 128), key_cache.reshape(SEQ, CACHE, 128),
        value_cache.reshape(SEQ, CACHE, 128), ffn_gain.reshape(1, D),
        routes.T, route_weight.T,
        expert_gate.reshape(D, 256), expert_up.reshape(D, 256), expert_down.reshape(256, D),
        dense_gate, dense_up, dense_down, gate_vector.reshape(1, 512),
    )


def solution(mesh):
    placed = (
        P("ep", None), P(), P(None, "tp"), P(None, "tp"), P(None, "tp"), P("tp", None), P(), P("tp"),
        P("ep", None, "tp", None), P("ep", None, "tp", None), P("ep"), P(), P("ep", None),
        P("ep", None), P("ep", None, "tp"), P("ep", None, "tp"), P("ep", "tp", None),
        P("tp", None), P("tp", None), P("tp", None), P("tp"),
    )
    return jax.shard_map(
        shards, mesh=mesh, in_specs=placed, out_specs=P("ep", "tp"), check_vma=False
    )
```

```python
import jax
import jax.numpy as jnp
from jax import lax
from jax.experimental import pallas as pl
from jax.experimental.pallas import tpu as pltpu
from jax.sharding import PartitionSpec as P

MESH = pl.DeviceIdType.MESH
BF = jnp.bfloat16
F32 = jnp.float32
EPS = 1e-06

SEQ = 16
D = 2048
QUARTER = 512
CACHE = 1024
NZ, NY, NC, NX = 8, 4, 2, 4
PEERS = NZ * NY * NC
ROWS = 2 * PEERS
ORDER = (0, 1, 7, 2, 6, 3, 5, 4)
PLACE = {dz: p for p, dz in enumerate(ORDER)}
CHUNKS = 4
CHUNK = ROWS // CHUNKS
GROUP = ROWS // NZ
BATCH = 4
HELD = (0, 2, 1, 3)
SWAPPED = ((0, 1, 1, 0), (0, 0, 1, 1))


def offsets(block):
    p, j = divmod(block, NY * NC)
    return ORDER[p], j // NC, j % NC


def opposite(block):
    dz, dy, dc = offsets(block)
    return PLACE[(NZ - dz) % NZ] * (NY * NC) + ((NY - dy) % NY) * NC + dc


def mm(a, b):
    return jnp.dot(a, b, preferred_element_type=F32)


def mm_t(a, b):
    return lax.dot_general(a, b, (((1,), (1,)), ((), ())), preferred_element_type=F32)


def silu(v):
    return v * (1.0 / (1.0 + jnp.exp(-v)))


def kernel(
    lambdas_h, lengths_h,
    tokens_h, norm_gain_h, wq_h, wk_h, wv_h, wo_h, head_gain_h, kc_h, vc_h, ffn_gain_h,
    routes_h, route_weight_h, eg_h, eu_h, ed_h, dg_h, du_h, dd_h, gate_h,
    out_ref,
    lambdas, lengths,
    tok, ng, wq, wk, wv, wo, hg, kc, vc, fg, rt, rw, eg, eu, ed, dg, du, dd, gv,
    qs, own, nv, sc, at, ho, near, far, ffn, outb, big, ungain,
    eparts, rs, rout, ret, ret2, dsend, drecv, gl, tick,
    load,
    p_send, p_recv, d_send, d_recv, ag_send, ag_recv, rs_send, rs_recv,
    b_send, b_recv, o_send, o_recv, ds_send, ds_recv, g_send, g_recv,
):
    me = lax.axis_index("ep")
    x = lax.axis_index("tp")
    z = lax.div(me, NY * NC)
    y = lax.rem(lax.div(me, NC), NY)
    c = lax.rem(me, NC)
    tps = [lax.rem(x + r, NX) for r in range(NX)]
    zs = [lax.rem(z + dz, NZ) * (NY * NC) for dz in range(NZ)]
    yc = [lax.rem(y + j // NC, NY) * NC + lax.rem(c + j % NC, NC) for j in range(NY * NC)]

    def ep_at(block):
        p, j = divmod(block, NY * NC)
        return zs[ORDER[p]] + yc[j]

    def quarter(r):
        return pl.ds(pl.multiple_of(tps[r] * QUARTER, QUARTER), QUARTER)

    def columns(r):
        return pl.ds(HELD.index(r) * QUARTER, QUARTER)

    def messages(count, sem):
        size = tick.at[pl.ds(0, count)]
        pltpu.make_async_copy(size, size, sem).wait()

    loads = []

    def fetch(src, dst):
        copy = pltpu.make_async_copy(src, dst, load.at[len(loads)])
        copy.start()
        loads.append(copy)
        return copy

    l_tok = fetch(tokens_h, tok)
    l_ng = fetch(norm_gain_h, ng)
    l_wq = fetch(wq_h, wq)
    l_wk = fetch(wk_h, wk)
    l_wv = fetch(wv_h, wv)
    parts = [pl.ds(i * BATCH, BATCH) for i in range(SEQ // BATCH)]
    keys = [fetch(kc_h.at[part], kc.at[part]) for part in parts]
    l_small = [
        fetch(lambdas_h, lambdas), fetch(lengths_h, lengths), fetch(head_gain_h, hg),
        fetch(ffn_gain_h, fg), fetch(routes_h, rt), fetch(route_weight_h, rw), fetch(gate_h, gv),
    ]
    values = [fetch(vc_h.at[part], vc.at[part]) for part in parts]
    l_wo = fetch(wo_h, wo)

    barrier = pltpu.get_barrier_semaphore()
    for r in (1, 2, 3):
        pl.semaphore_signal(barrier, inc=1, device_id=(me, tps[r]), device_id_type=MESH)
    for block in range(1, PEERS):
        there = ep_at(block)
        pl.semaphore_signal(barrier, inc=1, device_id=(there, x), device_id_type=MESH)
        pl.semaphore_signal(barrier, inc=1, device_id=(there, tps[2]), device_id_type=MESH)

    qs[...] = jnp.zeros((8 * SEQ, 128), F32)
    own[...] = jnp.zeros((8 * SEQ, 128), F32)
    l_tok.wait()
    l_ng.wait()
    wide = tok[...].astype(F32)
    scale = lax.rsqrt(jnp.mean(wide * wide, axis=-1, keepdims=True) + EPS)
    normed = (wide * scale * ng[...]).astype(BF)
    l_wq.wait()
    l_wk.wait()
    l_wv.wait()
    queries = mm(normed, wq[...]).astype(BF).astype(F32) * 0.125
    new_keys = mm(normed, wk[...]).astype(BF).astype(F32)
    nv[...] = mm(normed, wv[...]).astype(BF).astype(F32)
    low = lax.broadcasted_iota(jnp.int32, (SEQ, 128), 1) < 64
    even = (lax.broadcasted_iota(jnp.int32, (SEQ, 128), 0) & 1) == 0
    for m in range(2):
        for g in range(2):
            head = queries[:, g * 128 : (g + 1) * 128]
            head = jnp.where(low, head, 0.0) if m == 0 else jnp.where(low, 0.0, head)
            score = jnp.sum(head * new_keys, axis=-1, keepdims=True)
            score = jnp.broadcast_to(score, (SEQ, 128))
            for odd in range(2):
                r = (odd * 4 + m * 2 + g) * SEQ
                keep = jnp.logical_not(even) if odd else even
                qs[r : r + SEQ, :] = jnp.where(keep, head, 0.0)
                own[r : r + SEQ, :] = jnp.where(keep, score, 0.0)

    def of(ref, i):
        return ref[pl.ds(i, 8, stride=SEQ), :]

    for i in range(0, SEQ, 2):
        if i % BATCH == 0:
            keys[i // BATCH].wait()
        pair = mm_t(of(qs, i).astype(BF), kc[i])
        sc[i // 2] = pair + mm_t(of(qs, i + 1).astype(BF), kc[i + 1])
    l_dg = fetch(dg_h, dg)
    l_du = fetch(du_h, du)
    l_dd = fetch(dd_h, dd)
    l_eg = fetch(eg_h, eg)
    l_eu = fetch(eu_h, eu)
    l_ed = fetch(ed_h, ed)

    for copy in l_small:
        copy.wait()
    head_row = lax.broadcasted_iota(jnp.int32, (8, 1), 0)
    turn = head_row & 3
    sign = jnp.where(turn < 2, 1.0, jnp.where(turn == 2, -lambdas[0], -lambdas[1]))
    position = lax.broadcasted_iota(jnp.int32, (8, CACHE), 1)
    own_weights = []
    for i in range(0, SEQ, 2):
        live = jnp.where(head_row < 4, lengths[i], lengths[i + 1])
        scores = jnp.where(position < live, sc[i // 2], -jnp.inf)
        own_score = (of(own, i) + of(own, i + 1))[:, 0:1]
        top = jnp.maximum(jnp.max(scores, axis=-1, keepdims=True), own_score)
        probs = jnp.exp(scores - top)
        own_prob = jnp.exp(own_score - top)
        factor = sign / (jnp.sum(probs, axis=-1, keepdims=True) + own_prob)
        probs = probs * factor
        own_prob = own_prob * factor
        at[i // 2] = (probs + pltpu.roll(probs, 6, 0)).astype(BF)
        for first in (0, 4):
            both = own_prob[first : first + 2] + own_prob[first + 2 : first + 4]
            own_weights.append(both.astype(BF).astype(F32))

    for i in range(SEQ):
        if i % BATCH == 0:
            values[i // BATCH].wait()
        first = 4 * (i % 2)
        mixed = mm(at[i // 2], vc[i])[first : first + 2] + own_weights[i] * nv[i : i + 1, :]
        ho[i : i + 1, :] = mixed[0:1]
        ho[SEQ + i : SEQ + i + 1, :] = mixed[1:2]

    heads = ho[...]
    heads = heads * lax.rsqrt(jnp.mean(heads * heads, axis=-1, keepdims=True) + EPS) * hg[...]
    heads = heads.astype(BF)
    l_wo.wait()
    for ref, held in ((far, (1, 3)), (near, (0, 2))):
        for i, r in enumerate(held):
            share = mm(heads[:SEQ], wo[0:128, quarter(r)]) + mm(heads[SEQ:], wo[128:256, quarter(r)])
            ref[0, :, i * QUARTER : (i + 1) * QUARTER] = share.astype(BF)

    pl.semaphore_wait(barrier, 2 * (PEERS - 1) + NX - 1)

    def along_tp(r, src, dst, send, recv):
        return pltpu.make_async_remote_copy(
            src_ref=src, dst_ref=dst, send_sem=send, recv_sem=recv,
            device_id=(me, tps[r]), device_id_type=MESH,
        )

    shares = []

    def share_out(turn, r, src, dst):
        copy = along_tp(
            r, src.at[0], dst.at[NX - r], p_send.at[turn, r], p_recv.at[turn, NX - r]
        )
        copy.start()
        shares.append(copy)

    share_out(0, 1, far, near)
    share_out(0, 3, far, near)
    share_out(0, 2, near, near)
    share_out(1, 1, near, far)
    share_out(1, 3, near, far)
    share_out(1, 2, far, far)

    for r in HELD:
        ungain[:, columns(r)] = 1.0 / fg[:, quarter(r)]
    routes = rt[...]
    dz = ((routes >> 3) - z) & 7
    place = jnp.where(dz == 0, 0, jnp.where(dz <= 4, 2 * dz - 1, 16 - 2 * dz))
    dy = ((routes >> 1) - y) & 3
    dc = (routes - c) & 1
    rel = place * 8 + dy * 2 + dc
    row = lax.broadcasted_iota(jnp.int32, (ROWS, SEQ), 0)
    named = jnp.zeros((ROWS, SEQ), F32)
    weighted = jnp.zeros((ROWS, SEQ), F32)
    weights = rw[...]
    for k in range(4):
        hit = (row >> 1) == rel[k : k + 1, :]
        named = named + jnp.where(hit, 1.0, 0.0)
        weighted = weighted + jnp.where(hit, weights[k : k + 1, :], 0.0)
    before = lax.broadcasted_iota(jnp.int32, (SEQ, SEQ), 0) < lax.broadcasted_iota(
        jnp.int32, (SEQ, SEQ), 1
    )
    rank = mm(named.astype(BF), jnp.where(before, 1.0, 0.0).astype(BF))
    mine = jnp.abs(rank - (row & 1).astype(F32)) < 0.5
    dispatch = jnp.where(mine, named, 0.0).astype(BF)
    combine = jnp.where(mine, weighted, 0.0)

    def arrived_share(turn, ref, held):
        for r in (1, 3, 2):
            block = ref.at[r]
            pltpu.make_async_copy(block, block, p_recv.at[turn, r]).wait()
        half = []
        for i, r in enumerate(held):
            total = tok[:, quarter(r)].astype(F32)
            for sender in range(NX):
                swapped = SWAPPED[turn][sender]
                j = 1 - i if swapped else i
                total = total + ref[sender, :, j * QUARTER : (j + 1) * QUARTER].astype(F32)
            half.append(total)
            ffn[:, columns(r)] = (total * fg[:, quarter(r)]).astype(BF)
        return half

    first_half = arrived_share(0, near, (0, 2))
    outb[...] = mm(dispatch, ffn[:, 0 : 2 * QUARTER]).astype(BF)
    big[0:2, 0 : 2 * QUARTER] = outb[0:2, :]
    for block in reversed(range(1, PEERS)):
        there = opposite(block)
        pltpu.make_async_remote_copy(
            src_ref=outb.at[pl.ds(2 * block, 2), :],
            dst_ref=big.at[pl.ds(2 * there, 2), pl.ds(0, 2 * QUARTER)],
            send_sem=d_send,
            recv_sem=d_recv.at[there // (NY * NC)],
            device_id=(ep_at(block), x),
            device_id_type=MESH,
        ).start()

    second_half = arrived_share(1, far, (1, 3))
    squares = jnp.zeros((SEQ, 1), F32)
    for value in first_half + second_half:
        squares = squares + jnp.sum(value * value, axis=-1, keepdims=True)
    scale = lax.rsqrt(squares * (1.0 / D) + EPS)
    l_dg.wait()
    l_du.wait()
    pre = jnp.zeros((SEQ, 512), F32)
    up = jnp.zeros((SEQ, 512), F32)
    for r in HELD:
        block = ffn[:, columns(r)]
        pre = pre + mm_t(block, dg[:, quarter(r)])
        up = up + mm_t(block, du[:, quarter(r)])
    hidden = (silu(pre * scale) * (up * scale)).astype(BF)
    logit = jnp.sum(hidden.astype(F32) * gv[...], axis=-1, keepdims=True)
    gl[0] = jnp.broadcast_to(logit, (SEQ, 128))
    l_dd.wait()
    for r in range(NX):
        dsend[r] = mm(hidden, dd[:, quarter(r)]).astype(BF)
    for r in (2, 1, 3):
        copy = along_tp(r, dsend.at[r], drecv.at[NX - r], ds_send.at[r], ds_recv.at[NX - r])
        copy.start()
        shares.append(copy)
        copy = along_tp(r, gl.at[0], gl.at[NX - r], g_send.at[r], g_recv.at[NX - r])
        copy.start()
        shares.append(copy)

    def arrived(ch):
        for p in (2 * ch + 1, 2 * ch):
            messages(2 * GROUP - 4 * (p == 0), d_recv.at[p])
        rows = pl.ds(ch * CHUNK, CHUNK)
        for r in (1, 3):
            copy = along_tp(
                r, big.at[rows, columns(0)], big.at[rows, columns(NX - r)],
                ag_send.at[ch, r], ag_recv.at[ch, NX - r],
            )
            copy.start()
            shares.append(copy)

    def work(ch):
        rows = pl.ds(ch * CHUNK, CHUNK)
        for r in (1, 3):
            block = big.at[rows, columns(r)]
            pltpu.make_async_copy(block, block, ag_recv.at[ch, r]).wait()
        pre = jnp.zeros((CHUNK, 256), F32)
        up = jnp.zeros((CHUNK, 256), F32)
        squares = jnp.zeros((CHUNK, QUARTER), F32)
        for r in HELD:
            block = big[rows, columns(r)]
            pre = pre + mm(block, eg[quarter(r), :])
            up = up + mm(block, eu[quarter(r), :])
            value = block.astype(F32) * ungain[:, columns(r)]
            squares = squares + value * value
        row_scale = jnp.sum(squares, axis=-1, keepdims=True) * (1.0 / D)
        row_scale = lax.rsqrt(row_scale + EPS)
        hidden = (silu(pre * row_scale) * (up * row_scale)).astype(BF)
        for r in (1, 3, 2, 0):
            eparts[r, rows, :] = mm(hidden, ed[:, quarter(r)]).astype(BF)
        for r in (1, 3):
            copy = along_tp(
                r, eparts.at[r, rows, :], rs.at[NX - r, rows, :],
                rs_send.at[ch, r], rs_recv.at[ch, NX - r],
            )
            copy.start()
            shares.append(copy)

    def send_rows(src, dst, send, recv, tp, blocks):
        for block in reversed(blocks):
            pltpu.make_async_remote_copy(
                src_ref=src.at[pl.ds(2 * block, 2), :],
                dst_ref=dst.at[pl.ds(2 * opposite(block), 2), :],
                send_sem=send,
                recv_sem=recv,
                device_id=(ep_at(block), tp),
                device_id_type=MESH,
            ).start()

    def give_back(ch):
        rows = pl.ds(ch * CHUNK, CHUNK)
        total = eparts[0, rows, :].astype(F32)
        for r in (1, 3):
            block = rs.at[r, rows, :]
            pltpu.make_async_copy(block, block, rs_recv.at[ch, r]).wait()
            total = total + rs[r, rows, :].astype(F32)
        total = total.astype(BF)
        rout[rows, :] = total
        if ch == 0:
            ret[0:2, :] = total[0:2]
        send_rows(rout, ret, b_send, b_recv, x, range(max(1, ch * CHUNK // 2), (ch + 1) * CHUNK // 2))

    arrived(3)
    arrived(2)
    arrived(1)
    arrived(0)
    l_eg.wait()
    l_eu.wait()
    l_ed.wait()
    work(3)
    work(2)
    work(1)
    work(0)
    send_rows(eparts.at[2], ret2, o_send, o_recv, tps[2], range(PEERS))
    give_back(3)
    give_back(2)
    give_back(1)
    give_back(0)

    for r in (1, 3, 2):
        pltpu.make_async_copy(drecv.at[r], drecv.at[r], ds_recv.at[r]).wait()
        pltpu.make_async_copy(gl.at[r], gl.at[r], g_recv.at[r]).wait()
    dense = dsend[0].astype(F32)
    logit = gl[0]
    for r in (1, 2, 3):
        dense = dense + drecv[r].astype(F32)
        logit = logit + gl[r]
    gate = 1.0 / (1.0 + jnp.exp(-logit[:, 0:1]))
    kept = first_half[0] + gate * dense
    coarse = combine.astype(BF)
    fine = (combine - coarse.astype(F32)).astype(BF)

    messages(2 * PEERS, o_recv)
    messages(2 * PEERS - 2, b_recv)
    back = (ret[...].astype(F32) + ret2[...].astype(F32)).astype(BF)
    over = (((0,), (0,)), ((), ()))
    mix = lax.dot_general(coarse, back, over, preferred_element_type=F32)
    mix = mix + lax.dot_general(fine, back, over, preferred_element_type=F32)
    out_ref[...] = (kept + mix).astype(BF)

    for copy in shares:
        copy.wait_send()
    messages(4 * PEERS - 4, d_send)
    messages(2 * PEERS - 2, b_send)
    messages(2 * PEERS, o_send)


def shards(
    tokens, norm_gain, query_weight, key_weight, value_weight, output_weight, head_gain, lambdas,
    key_cache, value_cache, lengths, ffn_gain, routes, route_weight, expert_gate, expert_up,
    expert_down, dense_gate, dense_up, dense_down, gate_vector,
):
    hbm = pl.BlockSpec(memory_space=pl.ANY)
    vm = pltpu.VMEM
    dma = pltpu.SemaphoreType.DMA
    return pl.pallas_call(
        kernel,
        name="layer",
        out_shape=jax.ShapeDtypeStruct((SEQ, QUARTER), BF),
        in_specs=[hbm] * 21,
        out_specs=pl.BlockSpec(memory_space=pltpu.VMEM),
        scratch_shapes=[
            pltpu.SMEM((2,), F32), pltpu.SMEM((SEQ,), jnp.int32),
            vm((SEQ, D), BF), vm((1, D), F32), vm((D, 256), BF), vm((D, 128), BF), vm((D, 128), BF),
            vm((256, D), BF), vm((1, 128), F32), vm((SEQ, CACHE, 128), BF), vm((SEQ, CACHE, 128), BF),
            vm((1, D), F32), vm((4, SEQ), jnp.int32), vm((4, SEQ), F32),
            vm((D, 256), BF), vm((D, 256), BF), vm((256, D), BF),
            vm((512, D), BF), vm((512, D), BF), vm((512, D), BF), vm((1, 512), F32),
            vm((8 * SEQ, 128), F32), vm((8 * SEQ, 128), F32), vm((SEQ, 128), F32),
            vm((SEQ // 2, 8, CACHE), F32), vm((SEQ // 2, 8, CACHE), BF), vm((2 * SEQ, 128), F32),
            vm((NX, SEQ, 2 * QUARTER), BF), vm((NX, SEQ, 2 * QUARTER), BF), vm((SEQ, D), BF),
            vm((ROWS, 2 * QUARTER), BF), vm((ROWS, D), BF), vm((1, D), F32),
            vm((NX, ROWS, QUARTER), BF), vm((NX, ROWS, QUARTER), BF),
            vm((ROWS, QUARTER), BF), vm((ROWS, QUARTER), BF), vm((ROWS, QUARTER), BF),
            vm((NX, SEQ, QUARTER), BF), vm((NX, SEQ, QUARTER), BF), vm((NX, SEQ, 128), F32),
            vm((4 * PEERS, 2, 128), F32),
            dma((27,)),
            dma((2, NX)), dma((2, NX)), dma, dma((NZ,)),
            dma((CHUNKS, NX)), dma((CHUNKS, NX)), dma((CHUNKS, NX)), dma((CHUNKS, NX)),
            dma, dma, dma, dma, dma((NX,)), dma((NX,)), dma((NX,)), dma((NX,)),
        ],
        compiler_params=pltpu.CompilerParams(
            collective_id=0, has_side_effects=True, vmem_limit_bytes=60 * 1024 * 1024
        ),
    )(
        lambdas, lengths,
        tokens, norm_gain.reshape(1, D), query_weight, key_weight, value_weight, output_weight,
        head_gain.reshape(1, 128), key_cache.reshape(SEQ, CACHE, 128),
        value_cache.reshape(SEQ, CACHE, 128), ffn_gain.reshape(1, D),
        routes.T, route_weight.T,
        expert_gate.reshape(D, 256), expert_up.reshape(D, 256), expert_down.reshape(256, D),
        dense_gate, dense_up, dense_down, gate_vector.reshape(1, 512),
    )


def solution(mesh):
    placed = (
        P("ep", None), P(), P(None, "tp"), P(None, "tp"), P(None, "tp"), P("tp", None), P(), P("tp"),
        P("ep", None, "tp", None), P("ep", None, "tp", None), P("ep"), P(), P("ep", None),
        P("ep", None), P("ep", None, "tp"), P("ep", None, "tp"), P("ep", "tp", None),
        P("tp", None), P("tp", None), P("tp", None), P("tp"),
    )
    return jax.shard_map(
        shards, mesh=mesh, in_specs=placed, out_specs=P("ep", "tp"), check_vma=False
    )
```

```python
import jax
import jax.numpy as jnp
from jax import lax
from jax.experimental import pallas as pl
from jax.experimental.pallas import tpu as pltpu
from jax.sharding import PartitionSpec as P

MESH = pl.DeviceIdType.MESH
BF = jnp.bfloat16
F32 = jnp.float32
EPS = 1e-06

SEQ = 16
D = 2048
QUARTER = 512
CACHE = 1024
NZ, NY, NC, NX = 8, 4, 2, 4
PEERS = NZ * NY * NC
ROWS = 2 * PEERS
ORDER = (0, 1, 7, 2, 6, 3, 5, 4)
PLACE = {dz: p for p, dz in enumerate(ORDER)}
CHUNKS = 4
CHUNK = ROWS // CHUNKS
GROUP = ROWS // NZ
BATCH = 4
DIRECT = (True, True, True, False)
PARTNERS = {True: (1, 3), False: (2, 1, 3)}
HELD = (0, 2, 1, 3)
SWAPPED = ((0, 1, 1, 0), (0, 0, 1, 1))


def offsets(block):
    p, j = divmod(block, NY * NC)
    return ORDER[p], j // NC, j % NC


def opposite(block):
    dz, dy, dc = offsets(block)
    return PLACE[(NZ - dz) % NZ] * (NY * NC) + ((NY - dy) % NY) * NC + dc


def chunk_of(block):
    return 2 * block // CHUNK


def mm(a, b):
    return jnp.dot(a, b, preferred_element_type=F32)


def mm_t(a, b):
    return lax.dot_general(a, b, (((1,), (1,)), ((), ())), preferred_element_type=F32)


def silu(v):
    return v * (1.0 / (1.0 + jnp.exp(-v)))


def kernel(
    lambdas_h, lengths_h,
    tokens_h, norm_gain_h, wq_h, wk_h, wv_h, wo_h, head_gain_h, kc_h, vc_h, ffn_gain_h,
    routes_h, route_weight_h, eg_h, eu_h, ed_h, dg_h, du_h, dd_h, gate_h,
    out_ref,
    lambdas, lengths,
    tok, ng, wq, wk, wv, wo, hg, kc, vc, fg, rt, rw, eg, eu, ed, dg, du, dd, gv,
    qs, own, nv, sc, at, ho, near, far, ffn, outb, big, ungain,
    eparts, rs, rout, ret, ret2, dsend, drecv, gl, tick,
    load,
    p_send, p_recv, d_send, d_recv, ag_send, ag_recv, rs_send, rs_recv,
    b_send, b_recv, o_send, o_recv, ds_send, ds_recv, g_send, g_recv,
):
    me = lax.axis_index("ep")
    x = lax.axis_index("tp")
    z = lax.div(me, NY * NC)
    y = lax.rem(lax.div(me, NC), NY)
    c = lax.rem(me, NC)
    tps = [lax.rem(x + r, NX) for r in range(NX)]
    zs = [lax.rem(z + dz, NZ) * (NY * NC) for dz in range(NZ)]
    yc = [lax.rem(y + j // NC, NY) * NC + lax.rem(c + j % NC, NC) for j in range(NY * NC)]

    def ep_at(block):
        p, j = divmod(block, NY * NC)
        return zs[ORDER[p]] + yc[j]

    def quarter(r):
        return pl.ds(pl.multiple_of(tps[r] * QUARTER, QUARTER), QUARTER)

    def columns(r):
        return pl.ds(HELD.index(r) * QUARTER, QUARTER)

    def messages(count, sem):
        size = tick.at[pl.ds(0, count)]
        pltpu.make_async_copy(size, size, sem).wait()

    loads = []

    def fetch(src, dst):
        copy = pltpu.make_async_copy(src, dst, load.at[len(loads)])
        copy.start()
        loads.append(copy)
        return copy

    l_tok = fetch(tokens_h, tok)
    l_ng = fetch(norm_gain_h, ng)
    l_wq = fetch(wq_h, wq)
    l_wk = fetch(wk_h, wk)
    l_wv = fetch(wv_h, wv)
    parts = [pl.ds(i * BATCH, BATCH) for i in range(SEQ // BATCH)]
    keys = [fetch(kc_h.at[part], kc.at[part]) for part in parts]
    l_small = [
        fetch(lambdas_h, lambdas), fetch(lengths_h, lengths), fetch(head_gain_h, hg),
        fetch(ffn_gain_h, fg), fetch(routes_h, rt), fetch(route_weight_h, rw), fetch(gate_h, gv),
    ]
    values = [fetch(vc_h.at[part], vc.at[part]) for part in parts]
    l_wo = fetch(wo_h, wo)

    for p in range(NZ):
        if not DIRECT[chunk_of(opposite(p * NY * NC))]:
            ret2[p * GROUP : (p + 1) * GROUP, :] = jnp.zeros((GROUP, QUARTER), BF)

    barrier = pltpu.get_barrier_semaphore()
    for r in (1, 2, 3):
        pl.semaphore_signal(barrier, inc=1, device_id=(me, tps[r]), device_id_type=MESH)
    for block in reversed(range(1, PEERS)):
        there = ep_at(block)
        pl.semaphore_signal(barrier, inc=1, device_id=(there, x), device_id_type=MESH)
        pl.semaphore_signal(barrier, inc=1, device_id=(there, tps[2]), device_id_type=MESH)

    qs[...] = jnp.zeros((8 * SEQ, 128), F32)
    own[...] = jnp.zeros((8 * SEQ, 128), F32)
    l_tok.wait()
    l_ng.wait()
    wide = tok[...].astype(F32)
    scale = lax.rsqrt(jnp.mean(wide * wide, axis=-1, keepdims=True) + EPS)
    normed = (wide * scale * ng[...]).astype(BF)
    l_wq.wait()
    l_wk.wait()
    l_wv.wait()
    queries = mm(normed, wq[...]).astype(BF).astype(F32) * 0.125
    new_keys = mm(normed, wk[...]).astype(BF).astype(F32)
    nv[...] = mm(normed, wv[...]).astype(BF).astype(F32)
    low = lax.broadcasted_iota(jnp.int32, (SEQ, 128), 1) < 64
    even = (lax.broadcasted_iota(jnp.int32, (SEQ, 128), 0) & 1) == 0
    for m in range(2):
        for g in range(2):
            head = queries[:, g * 128 : (g + 1) * 128]
            head = jnp.where(low, head, 0.0) if m == 0 else jnp.where(low, 0.0, head)
            score = jnp.sum(head * new_keys, axis=-1, keepdims=True)
            score = jnp.broadcast_to(score, (SEQ, 128))
            for odd in range(2):
                r = (odd * 4 + m * 2 + g) * SEQ
                keep = jnp.logical_not(even) if odd else even
                qs[r : r + SEQ, :] = jnp.where(keep, head, 0.0)
                own[r : r + SEQ, :] = jnp.where(keep, score, 0.0)

    def of(ref, i):
        return ref[pl.ds(i, 8, stride=SEQ), :]

    for i in range(0, SEQ, 2):
        if i % BATCH == 0:
            keys[i // BATCH].wait()
        pair = mm_t(of(qs, i).astype(BF), kc[i])
        sc[i // 2] = pair + mm_t(of(qs, i + 1).astype(BF), kc[i + 1])
    l_dg = fetch(dg_h, dg)
    l_du = fetch(du_h, du)
    l_dd = fetch(dd_h, dd)
    l_eg = fetch(eg_h, eg)
    l_eu = fetch(eu_h, eu)
    l_ed = fetch(ed_h, ed)

    for copy in l_small:
        copy.wait()
    head_row = lax.broadcasted_iota(jnp.int32, (8, 1), 0)
    turn = head_row & 3
    sign = jnp.where(turn < 2, 1.0, jnp.where(turn == 2, -lambdas[0], -lambdas[1]))
    position = lax.broadcasted_iota(jnp.int32, (8, CACHE), 1)
    own_weights = []
    for i in range(0, SEQ, 2):
        live = jnp.where(head_row < 4, lengths[i], lengths[i + 1])
        scores = jnp.where(position < live, sc[i // 2], -jnp.inf)
        own_score = (of(own, i) + of(own, i + 1))[:, 0:1]
        top = jnp.maximum(jnp.max(scores, axis=-1, keepdims=True), own_score)
        probs = jnp.exp(scores - top)
        own_prob = jnp.exp(own_score - top)
        factor = sign / (jnp.sum(probs, axis=-1, keepdims=True) + own_prob)
        probs = probs * factor
        own_prob = own_prob * factor
        at[i // 2] = (probs + pltpu.roll(probs, 6, 0)).astype(BF)
        for first in (0, 4):
            both = own_prob[first : first + 2] + own_prob[first + 2 : first + 4]
            own_weights.append(both.astype(BF).astype(F32))

    for i in range(SEQ):
        if i % BATCH == 0:
            values[i // BATCH].wait()
        first = 4 * (i % 2)
        mixed = mm(at[i // 2], vc[i])[first : first + 2] + own_weights[i] * nv[i : i + 1, :]
        ho[i : i + 1, :] = mixed[0:1]
        ho[SEQ + i : SEQ + i + 1, :] = mixed[1:2]

    heads = ho[...]
    heads = heads * lax.rsqrt(jnp.mean(heads * heads, axis=-1, keepdims=True) + EPS) * hg[...]
    heads = heads.astype(BF)
    l_wo.wait()
    for ref, held in ((far, (1, 3)), (near, (0, 2))):
        for i, r in enumerate(held):
            share = mm(heads[:SEQ], wo[0:128, quarter(r)]) + mm(heads[SEQ:], wo[128:256, quarter(r)])
            ref[0, :, i * QUARTER : (i + 1) * QUARTER] = share.astype(BF)

    pl.semaphore_wait(barrier, 2 * (PEERS - 1) + NX - 1)

    def along_tp(r, src, dst, send, recv):
        return pltpu.make_async_remote_copy(
            src_ref=src, dst_ref=dst, send_sem=send, recv_sem=recv,
            device_id=(me, tps[r]), device_id_type=MESH,
        )

    shares = []

    def share_out(turn, r, src, dst):
        copy = along_tp(
            r, src.at[0], dst.at[NX - r], p_send.at[turn, r], p_recv.at[turn, NX - r]
        )
        copy.start()
        shares.append(copy)

    share_out(0, 1, far, near)
    share_out(0, 3, far, near)
    share_out(0, 2, near, near)
    share_out(1, 1, near, far)
    share_out(1, 3, near, far)
    share_out(1, 2, far, far)

    for r in HELD:
        ungain[:, columns(r)] = 1.0 / fg[:, quarter(r)]
    routes = rt[...]
    dz = ((routes >> 3) - z) & 7
    place = jnp.where(dz == 0, 0, jnp.where(dz <= 4, 2 * dz - 1, 16 - 2 * dz))
    dy = ((routes >> 1) - y) & 3
    dc = (routes - c) & 1
    rel = place * 8 + dy * 2 + dc
    row = lax.broadcasted_iota(jnp.int32, (ROWS, SEQ), 0)
    named = jnp.zeros((ROWS, SEQ), F32)
    weighted = jnp.zeros((ROWS, SEQ), F32)
    weights = rw[...]
    for k in range(4):
        hit = (row >> 1) == rel[k : k + 1, :]
        named = named + jnp.where(hit, 1.0, 0.0)
        weighted = weighted + jnp.where(hit, weights[k : k + 1, :], 0.0)
    before = lax.broadcasted_iota(jnp.int32, (SEQ, SEQ), 0) < lax.broadcasted_iota(
        jnp.int32, (SEQ, SEQ), 1
    )
    rank = mm(named.astype(BF), jnp.where(before, 1.0, 0.0).astype(BF))
    mine = jnp.abs(rank - (row & 1).astype(F32)) < 0.5
    dispatch = jnp.where(mine, named, 0.0).astype(BF)
    combine = jnp.where(mine, weighted, 0.0)

    def arrived_share(turn, ref, held):
        for r in (1, 3, 2):
            block = ref.at[r]
            pltpu.make_async_copy(block, block, p_recv.at[turn, r]).wait()
        half = []
        for i, r in enumerate(held):
            total = tok[:, quarter(r)].astype(F32)
            for sender in range(NX):
                swapped = SWAPPED[turn][sender]
                j = 1 - i if swapped else i
                total = total + ref[sender, :, j * QUARTER : (j + 1) * QUARTER].astype(F32)
            half.append(total)
            ffn[:, columns(r)] = (total * fg[:, quarter(r)]).astype(BF)
        return half

    first_half = arrived_share(0, near, (0, 2))
    outb[...] = mm(dispatch, ffn[:, 0 : 2 * QUARTER]).astype(BF)
    big[0:2, 0 : 2 * QUARTER] = outb[0:2, :]
    for block in reversed(range(1, PEERS)):
        there = opposite(block)
        width = pl.ds(0, 2 * QUARTER if DIRECT[chunk_of(there)] else QUARTER)
        pltpu.make_async_remote_copy(
            src_ref=outb.at[pl.ds(2 * block, 2), width],
            dst_ref=big.at[pl.ds(2 * there, 2), width],
            send_sem=d_send,
            recv_sem=d_recv.at[there // (NY * NC)],
            device_id=(ep_at(block), x),
            device_id_type=MESH,
        ).start()

    second_half = arrived_share(1, far, (1, 3))
    squares = jnp.zeros((SEQ, 1), F32)
    for value in first_half + second_half:
        squares = squares + jnp.sum(value * value, axis=-1, keepdims=True)
    scale = lax.rsqrt(squares * (1.0 / D) + EPS)
    l_dg.wait()
    l_du.wait()
    pre = jnp.zeros((SEQ, 512), F32)
    up = jnp.zeros((SEQ, 512), F32)
    for r in HELD:
        block = ffn[:, columns(r)]
        pre = pre + mm_t(block, dg[:, quarter(r)])
        up = up + mm_t(block, du[:, quarter(r)])
    hidden = (silu(pre * scale) * (up * scale)).astype(BF)
    logit = jnp.sum(hidden.astype(F32) * gv[...], axis=-1, keepdims=True)
    gl[0] = jnp.broadcast_to(logit, (SEQ, 128))
    l_dd.wait()
    for r in range(NX):
        dsend[r] = mm(hidden, dd[:, quarter(r)]).astype(BF)
    for r in (2, 1, 3):
        copy = along_tp(r, dsend.at[r], drecv.at[NX - r], ds_send.at[r], ds_recv.at[NX - r])
        copy.start()
        shares.append(copy)
        copy = along_tp(r, gl.at[0], gl.at[NX - r], g_send.at[r], g_recv.at[NX - r])
        copy.start()
        shares.append(copy)

    def arrived(ch):
        for p in (2 * ch + 1, 2 * ch):
            messages((GROUP // 2 - (p == 0)) * (4 if DIRECT[ch] else 2), d_recv.at[p])
        rows = pl.ds(ch * CHUNK, CHUNK)
        for r in PARTNERS[DIRECT[ch]]:
            copy = along_tp(
                r, big.at[rows, columns(0)], big.at[rows, columns(NX - r)],
                ag_send.at[ch, r], ag_recv.at[ch, NX - r],
            )
            copy.start()
            shares.append(copy)

    def work(ch):
        rows = pl.ds(ch * CHUNK, CHUNK)
        for r in PARTNERS[DIRECT[ch]]:
            block = big.at[rows, columns(r)]
            pltpu.make_async_copy(block, block, ag_recv.at[ch, r]).wait()
        pre = jnp.zeros((CHUNK, 256), F32)
        up = jnp.zeros((CHUNK, 256), F32)
        squares = jnp.zeros((CHUNK, QUARTER), F32)
        for r in HELD:
            block = big[rows, columns(r)]
            pre = pre + mm(block, eg[quarter(r), :])
            up = up + mm(block, eu[quarter(r), :])
            value = block.astype(F32) * ungain[:, columns(r)]
            squares = squares + value * value
        row_scale = jnp.sum(squares, axis=-1, keepdims=True) * (1.0 / D)
        row_scale = lax.rsqrt(row_scale + EPS)
        hidden = (silu(pre * row_scale) * (up * row_scale)).astype(BF)
        for r in (2, 1, 3, 0):
            eparts[r, rows, :] = mm(hidden, ed[:, quarter(r)]).astype(BF)
        for r in PARTNERS[DIRECT[ch]]:
            copy = along_tp(
                r, eparts.at[r, rows, :], rs.at[NX - r, rows, :],
                rs_send.at[ch, r], rs_recv.at[ch, NX - r],
            )
            copy.start()
            shares.append(copy)

    def send_rows(src, dst, send, recv, tp, blocks):
        for block in reversed(blocks):
            pltpu.make_async_remote_copy(
                src_ref=src.at[pl.ds(2 * block, 2), :],
                dst_ref=dst.at[pl.ds(2 * opposite(block), 2), :],
                send_sem=send,
                recv_sem=recv,
                device_id=(ep_at(block), tp),
                device_id_type=MESH,
            ).start()

    def give_back(ch):
        rows = pl.ds(ch * CHUNK, CHUNK)
        total = eparts[0, rows, :].astype(F32)
        for r in PARTNERS[DIRECT[ch]]:
            block = rs.at[r, rows, :]
            pltpu.make_async_copy(block, block, rs_recv.at[ch, r]).wait()
            total = total + rs[r, rows, :].astype(F32)
        total = total.astype(BF)
        rout[rows, :] = total
        if ch == 0:
            ret[0:2, :] = total[0:2]
        send_rows(rout, ret, b_send, b_recv, x, range(max(1, ch * CHUNK // 2), (ch + 1) * CHUNK // 2))

    def straight(ch):
        blocks = range(ch * CHUNK // 2, (ch + 1) * CHUNK // 2)
        send_rows(eparts.at[2], ret2, o_send, o_recv, tps[2], blocks)

    arrived(3)
    arrived(2)
    arrived(1)
    arrived(0)
    l_eg.wait()
    l_eu.wait()
    l_ed.wait()
    for ch in reversed(range(CHUNKS)):
        work(ch)
        if DIRECT[ch]:
            straight(ch)
    give_back(3)
    give_back(2)
    give_back(1)
    give_back(0)

    for r in (1, 3, 2):
        pltpu.make_async_copy(drecv.at[r], drecv.at[r], ds_recv.at[r]).wait()
        pltpu.make_async_copy(gl.at[r], gl.at[r], g_recv.at[r]).wait()
    dense = dsend[0].astype(F32)
    logit = gl[0]
    for r in (1, 2, 3):
        dense = dense + drecv[r].astype(F32)
        logit = logit + gl[r]
    gate = 1.0 / (1.0 + jnp.exp(-logit[:, 0:1]))
    kept = first_half[0] + gate * dense
    coarse = combine.astype(BF)
    fine = (combine - coarse.astype(F32)).astype(BF)

    messages(DIRECT.count(True) * CHUNK, o_recv)
    messages(2 * PEERS - 2, b_recv)
    back = (ret[...].astype(F32) + ret2[...].astype(F32)).astype(BF)
    over = (((0,), (0,)), ((), ()))
    mix = lax.dot_general(coarse, back, over, preferred_element_type=F32)
    mix = mix + lax.dot_general(fine, back, over, preferred_element_type=F32)
    out_ref[...] = (kept + mix).astype(BF)

    for copy in shares:
        copy.wait_send()
    messages(sum(4 if DIRECT[chunk_of(opposite(b))] else 2 for b in range(1, PEERS)), d_send)
    messages(2 * PEERS - 2, b_send)
    messages(DIRECT.count(True) * CHUNK, o_send)


def shards(
    tokens, norm_gain, query_weight, key_weight, value_weight, output_weight, head_gain, lambdas,
    key_cache, value_cache, lengths, ffn_gain, routes, route_weight, expert_gate, expert_up,
    expert_down, dense_gate, dense_up, dense_down, gate_vector,
):
    hbm = pl.BlockSpec(memory_space=pltpu.HBM)
    vm = pltpu.VMEM
    dma = pltpu.SemaphoreType.DMA
    return pl.pallas_call(
        kernel,
        name="layer",
        out_shape=jax.ShapeDtypeStruct((SEQ, QUARTER), BF),
        in_specs=[hbm] * 21,
        out_specs=pl.BlockSpec(memory_space=pltpu.VMEM),
        scratch_shapes=[
            pltpu.SMEM((2,), F32), pltpu.SMEM((SEQ,), jnp.int32),
            vm((SEQ, D), BF), vm((1, D), F32), vm((D, 256), BF), vm((D, 128), BF), vm((D, 128), BF),
            vm((256, D), BF), vm((1, 128), F32), vm((SEQ, CACHE, 128), BF), vm((SEQ, CACHE, 128), BF),
            vm((1, D), F32), vm((4, SEQ), jnp.int32), vm((4, SEQ), F32),
            vm((D, 256), BF), vm((D, 256), BF), vm((256, D), BF),
            vm((512, D), BF), vm((512, D), BF), vm((512, D), BF), vm((1, 512), F32),
            vm((8 * SEQ, 128), F32), vm((8 * SEQ, 128), F32), vm((SEQ, 128), F32),
            vm((SEQ // 2, 8, CACHE), F32), vm((SEQ // 2, 8, CACHE), BF), vm((2 * SEQ, 128), F32),
            vm((NX, SEQ, 2 * QUARTER), BF), vm((NX, SEQ, 2 * QUARTER), BF), vm((SEQ, D), BF),
            vm((ROWS, 2 * QUARTER), BF), vm((ROWS, D), BF), vm((1, D), F32),
            vm((NX, ROWS, QUARTER), BF), vm((NX, ROWS, QUARTER), BF),
            vm((ROWS, QUARTER), BF), vm((ROWS, QUARTER), BF), vm((ROWS, QUARTER), BF),
            vm((NX, SEQ, QUARTER), BF), vm((NX, SEQ, QUARTER), BF), vm((NX, SEQ, 128), F32),
            vm((4 * PEERS, 2, 128), F32),
            dma((27,)),
            dma((2, NX)), dma((2, NX)), dma, dma((NZ,)),
            dma((CHUNKS, NX)), dma((CHUNKS, NX)), dma((CHUNKS, NX)), dma((CHUNKS, NX)),
            dma, dma, dma, dma, dma((NX,)), dma((NX,)), dma((NX,)), dma((NX,)),
        ],
        compiler_params=pltpu.CompilerParams(
            collective_id=0, has_side_effects=True, vmem_limit_bytes=50 * 1024 * 1024
        ),
    )(*[pltpu.with_memory_space_constraint(operand, pltpu.HBM) for operand in (
        lambdas, lengths,
        tokens, norm_gain.reshape(1, D), query_weight, key_weight, value_weight, output_weight,
        head_gain.reshape(1, 128), key_cache.reshape(SEQ, CACHE, 128),
        value_cache.reshape(SEQ, CACHE, 128), ffn_gain.reshape(1, D),
        routes.T, route_weight.T,
        expert_gate.reshape(D, 256), expert_up.reshape(D, 256), expert_down.reshape(256, D),
        dense_gate, dense_up, dense_down, gate_vector.reshape(1, 512),
    )])


def solution(mesh):
    placed = (
        P("ep", None), P(), P(None, "tp"), P(None, "tp"), P(None, "tp"), P("tp", None), P(), P("tp"),
        P("ep", None, "tp", None), P("ep", None, "tp", None), P("ep"), P(), P("ep", None),
        P("ep", None), P("ep", None, "tp"), P("ep", None, "tp"), P("ep", "tp", None),
        P("tp", None), P("tp", None), P("tp", None), P("tp"),
    )
    return jax.shard_map(
        shards, mesh=mesh, in_specs=placed, out_specs=P("ep", "tp"), check_vma=False
    )
```

```python
import jax
import jax.numpy as jnp
from jax import lax
from jax.experimental import pallas as pl
from jax.experimental.pallas import tpu as pltpu
from jax.sharding import PartitionSpec as P

MESH = pl.DeviceIdType.MESH
BF = jnp.bfloat16
F32 = jnp.float32
EPS = 1e-06

SEQ = 16
D = 2048
QUARTER = 512
CACHE = 1024
NZ, NY, NC, NX = 8, 4, 2, 4
PEERS = NZ * NY * NC
ROWS = 2 * PEERS
ORDER = (0, 1, 7, 2, 6, 3, 5, 4)
PLACE = {dz: p for p, dz in enumerate(ORDER)}
CHUNKS = 4
CHUNK = ROWS // CHUNKS
GROUP = ROWS // NZ
BATCH = 4
DIRECT = (True, True, True, False)
PARTNERS = {True: (1, 3), False: (2, 1, 3)}
HELD = (0, 2, 1, 3)
SWAPPED = ((0, 1, 1, 0), (0, 0, 1, 1))


def offsets(block):
    p, j = divmod(block, NY * NC)
    return ORDER[p], j // NC, j % NC


def opposite(block):
    dz, dy, dc = offsets(block)
    return PLACE[(NZ - dz) % NZ] * (NY * NC) + ((NY - dy) % NY) * NC + dc


def chunk_of(block):
    return 2 * block // CHUNK


def mm(a, b):
    return jnp.dot(a, b, preferred_element_type=F32)


def mm_t(a, b):
    return lax.dot_general(a, b, (((1,), (1,)), ((), ())), preferred_element_type=F32)


def silu(v):
    return v * (1.0 / (1.0 + jnp.exp(-v)))


def kernel(
    lambdas_h, lengths_h,
    tokens_h, norm_gain_h, wq_h, wk_h, wv_h, wo_h, head_gain_h, kc_h, vc_h, ffn_gain_h,
    routes_h, route_weight_h, eg_h, eu_h, ed_h, dg_h, du_h, dd_h, gate_h,
    out_ref,
    lambdas, lengths,
    tok, ng, wq, wk, wv, wo, hg, kc, vc, fg, rt, rw, eg, eu, ed, dg, du, dd, gv,
    qs, own, nv, sc, at, ho, near, far, ffn, outb, big, ungain,
    eparts, rs, rout, ret, ret2, dsend, drecv, gl, tick,
    load,
    p_send, p_recv, d_send, d_recv, ag_send, ag_recv, rs_send, rs_recv,
    b_send, b_recv, o_send, o_recv, ds_send, ds_recv, g_send, g_recv,
):
    me = lax.axis_index("ep")
    x = lax.axis_index("tp")
    z = lax.div(me, NY * NC)
    y = lax.rem(lax.div(me, NC), NY)
    c = lax.rem(me, NC)
    tps = [lax.rem(x + r, NX) for r in range(NX)]
    zs = [lax.rem(z + dz, NZ) * (NY * NC) for dz in range(NZ)]
    yc = [lax.rem(y + j // NC, NY) * NC + lax.rem(c + j % NC, NC) for j in range(NY * NC)]

    def ep_at(block):
        p, j = divmod(block, NY * NC)
        return zs[ORDER[p]] + yc[j]

    def quarter(r):
        return pl.ds(pl.multiple_of(tps[r] * QUARTER, QUARTER), QUARTER)

    def columns(r):
        return pl.ds(HELD.index(r) * QUARTER, QUARTER)

    def messages(count, sem):
        size = tick.at[pl.ds(0, count)]
        pltpu.make_async_copy(size, size, sem).wait()

    loads = []

    def fetch(src, dst):
        copy = pltpu.make_async_copy(src, dst, load.at[len(loads)])
        copy.start()
        loads.append(copy)
        return copy

    l_tok = fetch(tokens_h, tok)
    l_ng = fetch(norm_gain_h, ng)
    l_wq = fetch(wq_h, wq)
    l_wk = fetch(wk_h, wk)
    l_wv = fetch(wv_h, wv)
    parts = [pl.ds(i * BATCH, BATCH) for i in range(SEQ // BATCH)]
    keys = [fetch(kc_h.at[part], kc.at[part]) for part in parts]
    l_small = [
        fetch(lambdas_h, lambdas), fetch(lengths_h, lengths), fetch(head_gain_h, hg),
        fetch(ffn_gain_h, fg), fetch(routes_h, rt), fetch(route_weight_h, rw), fetch(gate_h, gv),
    ]
    values = [fetch(vc_h.at[part], vc.at[part]) for part in parts]
    l_wo = fetch(wo_h, wo)

    for p in range(NZ):
        if not DIRECT[chunk_of(opposite(p * NY * NC))]:
            ret2[p * GROUP : (p + 1) * GROUP, :] = jnp.zeros((GROUP, QUARTER), BF)

    barrier = pltpu.get_barrier_semaphore()
    for r in (1, 2, 3):
        pl.semaphore_signal(barrier, inc=1, device_id=(me, tps[r]), device_id_type=MESH)
    for block in reversed(range(1, PEERS)):
        there = ep_at(block)
        pl.semaphore_signal(barrier, inc=1, device_id=(there, x), device_id_type=MESH)
        if DIRECT[chunk_of(block)] or DIRECT[chunk_of(opposite(block))]:
            pl.semaphore_signal(barrier, inc=1, device_id=(there, tps[2]), device_id_type=MESH)

    qs[...] = jnp.zeros((8 * SEQ, 128), F32)
    own[...] = jnp.zeros((8 * SEQ, 128), F32)
    l_tok.wait()
    l_ng.wait()
    wide = tok[...].astype(F32)
    scale = lax.rsqrt(jnp.mean(wide * wide, axis=-1, keepdims=True) + EPS)
    normed = (wide * scale * ng[...]).astype(BF)
    l_wq.wait()
    l_wk.wait()
    l_wv.wait()
    queries = mm(normed, wq[...]).astype(BF).astype(F32) * 0.125
    new_keys = mm(normed, wk[...]).astype(BF).astype(F32)
    nv[...] = mm(normed, wv[...]).astype(BF).astype(F32)
    low = lax.broadcasted_iota(jnp.int32, (SEQ, 128), 1) < 64
    even = (lax.broadcasted_iota(jnp.int32, (SEQ, 128), 0) & 1) == 0
    for m in range(2):
        for g in range(2):
            head = queries[:, g * 128 : (g + 1) * 128]
            head = jnp.where(low, head, 0.0) if m == 0 else jnp.where(low, 0.0, head)
            score = jnp.sum(head * new_keys, axis=-1, keepdims=True)
            score = jnp.broadcast_to(score, (SEQ, 128))
            for odd in range(2):
                r = (odd * 4 + m * 2 + g) * SEQ
                keep = jnp.logical_not(even) if odd else even
                qs[r : r + SEQ, :] = jnp.where(keep, head, 0.0)
                own[r : r + SEQ, :] = jnp.where(keep, score, 0.0)

    def of(ref, i):
        return ref[pl.ds(i, 8, stride=SEQ), :]

    for i in range(0, SEQ, 2):
        if i % BATCH == 0:
            keys[i // BATCH].wait()
        pair = mm_t(of(qs, i).astype(BF), kc[i])
        sc[i // 2] = pair + mm_t(of(qs, i + 1).astype(BF), kc[i + 1])
    l_dg = fetch(dg_h, dg)
    l_du = fetch(du_h, du)
    l_dd = fetch(dd_h, dd)
    l_eg = fetch(eg_h, eg)
    l_eu = fetch(eu_h, eu)
    l_ed = fetch(ed_h, ed)

    for copy in l_small:
        copy.wait()
    head_row = lax.broadcasted_iota(jnp.int32, (8, 1), 0)
    turn = head_row & 3
    sign = jnp.where(turn < 2, 1.0, jnp.where(turn == 2, -lambdas[0], -lambdas[1]))
    position = lax.broadcasted_iota(jnp.int32, (8, CACHE), 1)
    own_weights = []
    for i in range(0, SEQ, 2):
        live = jnp.where(head_row < 4, lengths[i], lengths[i + 1])
        scores = jnp.where(position < live, sc[i // 2], -jnp.inf)
        own_score = (of(own, i) + of(own, i + 1))[:, 0:1]
        top = jnp.maximum(jnp.max(scores, axis=-1, keepdims=True), own_score)
        probs = jnp.exp(scores - top)
        own_prob = jnp.exp(own_score - top)
        factor = sign / (jnp.sum(probs, axis=-1, keepdims=True) + own_prob)
        probs = probs * factor
        own_prob = own_prob * factor
        at[i // 2] = (probs + pltpu.roll(probs, 6, 0)).astype(BF)
        for first in (0, 4):
            both = own_prob[first : first + 2] + own_prob[first + 2 : first + 4]
            own_weights.append(both.astype(BF).astype(F32))

    for i in range(SEQ):
        if i % BATCH == 0:
            values[i // BATCH].wait()
        first = 4 * (i % 2)
        mixed = mm(at[i // 2], vc[i])[first : first + 2] + own_weights[i] * nv[i : i + 1, :]
        ho[i : i + 1, :] = mixed[0:1]
        ho[SEQ + i : SEQ + i + 1, :] = mixed[1:2]

    heads = ho[...]
    heads = heads * lax.rsqrt(jnp.mean(heads * heads, axis=-1, keepdims=True) + EPS) * hg[...]
    heads = heads.astype(BF)
    l_wo.wait()
    for ref, held in ((far, (1, 3)), (near, (0, 2))):
        for i, r in enumerate(held):
            share = mm(heads[:SEQ], wo[0:128, quarter(r)]) + mm(heads[SEQ:], wo[128:256, quarter(r)])
            ref[0, :, i * QUARTER : (i + 1) * QUARTER] = share.astype(BF)

    straight_partners = sum(DIRECT[chunk_of(b)] or DIRECT[chunk_of(opposite(b))] for b in range(1, PEERS))
    pl.semaphore_wait(barrier, PEERS - 1 + straight_partners + NX - 1)

    def along_tp(r, src, dst, send, recv):
        return pltpu.make_async_remote_copy(
            src_ref=src, dst_ref=dst, send_sem=send, recv_sem=recv,
            device_id=(me, tps[r]), device_id_type=MESH,
        )

    shares = []

    def share_out(turn, r, src, dst):
        copy = along_tp(
            r, src.at[0], dst.at[NX - r], p_send.at[turn, r], p_recv.at[turn, NX - r]
        )
        copy.start()
        shares.append(copy)

    share_out(0, 2, near, near)
    share_out(0, 1, far, near)
    share_out(0, 3, far, near)
    share_out(1, 1, near, far)
    share_out(1, 3, near, far)
    share_out(1, 2, far, far)

    for r in HELD:
        ungain[:, columns(r)] = 1.0 / fg[:, quarter(r)]
    routes = rt[...]
    dz = ((routes >> 3) - z) & 7
    place = jnp.where(dz == 0, 0, jnp.where(dz <= 4, 2 * dz - 1, 16 - 2 * dz))
    dy = ((routes >> 1) - y) & 3
    dc = (routes - c) & 1
    rel = place * 8 + dy * 2 + dc
    row = lax.broadcasted_iota(jnp.int32, (ROWS, SEQ), 0)
    named = jnp.zeros((ROWS, SEQ), F32)
    weighted = jnp.zeros((ROWS, SEQ), F32)
    weights = rw[...]
    for k in range(4):
        hit = (row >> 1) == rel[k : k + 1, :]
        named = named + jnp.where(hit, 1.0, 0.0)
        weighted = weighted + jnp.where(hit, weights[k : k + 1, :], 0.0)
    before = lax.broadcasted_iota(jnp.int32, (SEQ, SEQ), 0) < lax.broadcasted_iota(
        jnp.int32, (SEQ, SEQ), 1
    )
    rank = mm(named.astype(BF), jnp.where(before, 1.0, 0.0).astype(BF))
    mine = jnp.abs(rank - (row & 1).astype(F32)) < 0.5
    dispatch = jnp.where(mine, named, 0.0).astype(BF)
    combine = jnp.where(mine, weighted, 0.0)

    def arrived_share(turn, ref, held):
        for r in (1, 3, 2):
            block = ref.at[r]
            pltpu.make_async_copy(block, block, p_recv.at[turn, r]).wait()
        half = []
        for i, r in enumerate(held):
            total = tok[:, quarter(r)].astype(F32)
            for sender in range(NX):
                swapped = SWAPPED[turn][sender]
                j = 1 - i if swapped else i
                total = total + ref[sender, :, j * QUARTER : (j + 1) * QUARTER].astype(F32)
            half.append(total)
            ffn[:, columns(r)] = (total * fg[:, quarter(r)]).astype(BF)
        return half

    first_half = arrived_share(0, near, (0, 2))
    outb[...] = mm(dispatch, ffn[:, 0 : 2 * QUARTER]).astype(BF)
    big[0:2, 0 : 2 * QUARTER] = outb[0:2, :]
    for block in reversed(range(1, PEERS)):
        there = opposite(block)
        width = pl.ds(0, 2 * QUARTER if DIRECT[chunk_of(there)] else QUARTER)
        pltpu.make_async_remote_copy(
            src_ref=outb.at[pl.ds(2 * block, 2), width],
            dst_ref=big.at[pl.ds(2 * there, 2), width],
            send_sem=d_send,
            recv_sem=d_recv.at[there // (NY * NC)],
            device_id=(ep_at(block), x),
            device_id_type=MESH,
        ).start()

    second_half = arrived_share(1, far, (1, 3))
    squares = jnp.zeros((SEQ, 1), F32)
    for value in first_half + second_half:
        squares = squares + jnp.sum(value * value, axis=-1, keepdims=True)
    scale = lax.rsqrt(squares * (1.0 / D) + EPS)
    l_dg.wait()
    l_du.wait()
    pre = jnp.zeros((SEQ, 512), F32)
    up = jnp.zeros((SEQ, 512), F32)
    for r in HELD:
        block = ffn[:, columns(r)]
        pre = pre + mm_t(block, dg[:, quarter(r)])
        up = up + mm_t(block, du[:, quarter(r)])
    hidden = (silu(pre * scale) * (up * scale)).astype(BF)
    logit = jnp.sum(hidden.astype(F32) * gv[...], axis=-1, keepdims=True)
    gl[0] = jnp.broadcast_to(logit, (SEQ, 128))
    l_dd.wait()
    for r in range(NX):
        dsend[r] = mm(hidden, dd[:, quarter(r)]).astype(BF)
    for r in (2, 1, 3):
        copy = along_tp(r, dsend.at[r], drecv.at[NX - r], ds_send.at[r], ds_recv.at[NX - r])
        copy.start()
        shares.append(copy)
        copy = along_tp(r, gl.at[0], gl.at[NX - r], g_send.at[r], g_recv.at[NX - r])
        copy.start()
        shares.append(copy)

    def arrived(ch):
        for p in (2 * ch + 1, 2 * ch):
            messages((GROUP // 2 - (p == 0)) * (4 if DIRECT[ch] else 2), d_recv.at[p])
        rows = pl.ds(ch * CHUNK, CHUNK)
        for r in PARTNERS[DIRECT[ch]]:
            copy = along_tp(
                r, big.at[rows, columns(0)], big.at[rows, columns(NX - r)],
                ag_send.at[ch, r], ag_recv.at[ch, NX - r],
            )
            copy.start()
            shares.append(copy)

    def work(ch):
        rows = pl.ds(ch * CHUNK, CHUNK)
        for r in PARTNERS[DIRECT[ch]]:
            block = big.at[rows, columns(r)]
            pltpu.make_async_copy(block, block, ag_recv.at[ch, r]).wait()
        pre = jnp.zeros((CHUNK, 256), F32)
        up = jnp.zeros((CHUNK, 256), F32)
        squares = jnp.zeros((CHUNK, QUARTER), F32)
        for r in HELD:
            block = big[rows, columns(r)]
            pre = pre + mm(block, eg[quarter(r), :])
            up = up + mm(block, eu[quarter(r), :])
            value = block.astype(F32) * ungain[:, columns(r)]
            squares = squares + value * value
        row_scale = jnp.sum(squares, axis=-1, keepdims=True) * (1.0 / D)
        row_scale = lax.rsqrt(row_scale + EPS)
        hidden = (silu(pre * row_scale) * (up * row_scale)).astype(BF)
        for r in (2, 1, 3, 0):
            eparts[r, rows, :] = mm(hidden, ed[:, quarter(r)]).astype(BF)
        for r in PARTNERS[DIRECT[ch]]:
            copy = along_tp(
                r, eparts.at[r, rows, :], rs.at[NX - r, rows, :],
                rs_send.at[ch, r], rs_recv.at[ch, NX - r],
            )
            copy.start()
            shares.append(copy)

    def send_rows(src, dst, send, recv, tp, blocks):
        for block in reversed(blocks):
            pltpu.make_async_remote_copy(
                src_ref=src.at[pl.ds(2 * block, 2), :],
                dst_ref=dst.at[pl.ds(2 * opposite(block), 2), :],
                send_sem=send,
                recv_sem=recv,
                device_id=(ep_at(block), tp),
                device_id_type=MESH,
            ).start()

    def give_back(ch):
        rows = pl.ds(ch * CHUNK, CHUNK)
        total = eparts[0, rows, :].astype(F32)
        for r in PARTNERS[DIRECT[ch]]:
            block = rs.at[r, rows, :]
            pltpu.make_async_copy(block, block, rs_recv.at[ch, r]).wait()
            total = total + rs[r, rows, :].astype(F32)
        total = total.astype(BF)
        rout[rows, :] = total
        if ch == 0:
            ret[0:2, :] = total[0:2]
        send_rows(rout, ret, b_send, b_recv, x, range(max(1, ch * CHUNK // 2), (ch + 1) * CHUNK // 2))

    def straight(ch):
        blocks = range(ch * CHUNK // 2, (ch + 1) * CHUNK // 2)
        send_rows(eparts.at[2], ret2, o_send, o_recv, tps[2], blocks)

    arrived(3)
    arrived(2)
    arrived(1)
    arrived(0)
    l_eg.wait()
    l_eu.wait()
    l_ed.wait()
    work(3)
    work(2)
    work(1)
    work(0)
    straight(2)
    straight(1)
    straight(0)
    give_back(3)
    give_back(2)
    give_back(1)
    give_back(0)

    for r in (1, 3, 2):
        pltpu.make_async_copy(drecv.at[r], drecv.at[r], ds_recv.at[r]).wait()
        pltpu.make_async_copy(gl.at[r], gl.at[r], g_recv.at[r]).wait()
    dense = dsend[0].astype(F32)
    logit = gl[0]
    for r in (1, 2, 3):
        dense = dense + drecv[r].astype(F32)
        logit = logit + gl[r]
    gate = 1.0 / (1.0 + jnp.exp(-logit[:, 0:1]))
    kept = first_half[0] + gate * dense
    coarse = combine.astype(BF)
    fine = (combine - coarse.astype(F32)).astype(BF)

    messages(DIRECT.count(True) * CHUNK, o_recv)
    messages(2 * PEERS - 2, b_recv)
    back = (ret[...].astype(F32) + ret2[...].astype(F32)).astype(BF)
    over = (((0,), (0,)), ((), ()))
    mix = lax.dot_general(coarse, back, over, preferred_element_type=F32)
    mix = mix + lax.dot_general(fine, back, over, preferred_element_type=F32)
    out_ref[...] = (kept + mix).astype(BF)

    for copy in shares:
        copy.wait_send()
    messages(sum(4 if DIRECT[chunk_of(opposite(b))] else 2 for b in range(1, PEERS)), d_send)
    messages(2 * PEERS - 2, b_send)
    messages(DIRECT.count(True) * CHUNK, o_send)


def shards(
    tokens, norm_gain, query_weight, key_weight, value_weight, output_weight, head_gain, lambdas,
    key_cache, value_cache, lengths, ffn_gain, routes, route_weight, expert_gate, expert_up,
    expert_down, dense_gate, dense_up, dense_down, gate_vector,
):
    hbm = pl.BlockSpec(memory_space=pltpu.HBM)
    vm = pltpu.VMEM
    dma = pltpu.SemaphoreType.DMA
    return pl.pallas_call(
        kernel,
        name="layer",
        out_shape=jax.ShapeDtypeStruct((SEQ, QUARTER), BF),
        in_specs=[hbm] * 21,
        out_specs=pl.BlockSpec(memory_space=pltpu.VMEM),
        scratch_shapes=[
            pltpu.SMEM((2,), F32), pltpu.SMEM((SEQ,), jnp.int32),
            vm((SEQ, D), BF), vm((1, D), F32), vm((D, 256), BF), vm((D, 128), BF), vm((D, 128), BF),
            vm((256, D), BF), vm((1, 128), F32), vm((SEQ, CACHE, 128), BF), vm((SEQ, CACHE, 128), BF),
            vm((1, D), F32), vm((4, SEQ), jnp.int32), vm((4, SEQ), F32),
            vm((D, 256), BF), vm((D, 256), BF), vm((256, D), BF),
            vm((512, D), BF), vm((512, D), BF), vm((512, D), BF), vm((1, 512), F32),
            vm((8 * SEQ, 128), F32), vm((8 * SEQ, 128), F32), vm((SEQ, 128), F32),
            vm((SEQ // 2, 8, CACHE), F32), vm((SEQ // 2, 8, CACHE), BF), vm((2 * SEQ, 128), F32),
            vm((NX, SEQ, 2 * QUARTER), BF), vm((NX, SEQ, 2 * QUARTER), BF), vm((SEQ, D), BF),
            vm((ROWS, 2 * QUARTER), BF), vm((ROWS, D), BF), vm((1, D), F32),
            vm((NX, ROWS, QUARTER), BF), vm((NX, ROWS, QUARTER), BF),
            vm((ROWS, QUARTER), BF), vm((ROWS, QUARTER), BF), vm((ROWS, QUARTER), BF),
            vm((NX, SEQ, QUARTER), BF), vm((NX, SEQ, QUARTER), BF), vm((NX, SEQ, 128), F32),
            vm((4 * PEERS, 2, 128), F32),
            dma((27,)),
            dma((2, NX)), dma((2, NX)), dma, dma((NZ,)),
            dma((CHUNKS, NX)), dma((CHUNKS, NX)), dma((CHUNKS, NX)), dma((CHUNKS, NX)),
            dma, dma, dma, dma, dma((NX,)), dma((NX,)), dma((NX,)), dma((NX,)),
        ],
        compiler_params=pltpu.CompilerParams(
            collective_id=0, has_side_effects=True, vmem_limit_bytes=50 * 1024 * 1024
        ),
    )(*[pltpu.with_memory_space_constraint(operand, pltpu.HBM) for operand in (
        lambdas, lengths,
        tokens, norm_gain.reshape(1, D), query_weight, key_weight, value_weight, output_weight,
        head_gain.reshape(1, 128), key_cache.reshape(SEQ, CACHE, 128),
        value_cache.reshape(SEQ, CACHE, 128), ffn_gain.reshape(1, D),
        routes.T, route_weight.T,
        expert_gate.reshape(D, 256), expert_up.reshape(D, 256), expert_down.reshape(256, D),
        dense_gate, dense_up, dense_down, gate_vector.reshape(1, 512),
    )])


def solution(mesh):
    placed = (
        P("ep", None), P(), P(None, "tp"), P(None, "tp"), P(None, "tp"), P("tp", None), P(), P("tp"),
        P("ep", None, "tp", None), P("ep", None, "tp", None), P("ep"), P(), P("ep", None),
        P("ep", None), P("ep", None, "tp"), P("ep", None, "tp"), P("ep", "tp", None),
        P("tp", None), P("tp", None), P("tp", None), P("tp"),
    )
    return jax.shard_map(
        shards, mesh=mesh, in_specs=placed, out_specs=P("ep", "tp"), check_vma=False
    )
```
